32 devices in a mesh: ep: 8 (over z, y), tp: 4 (over x, core).
Axes of the slice: x: 2, y: 2, z: 4, core: 2. Of those that a mesh axis runs over, the one named last changes fastest.
Arguments:
- q_latent: bfloat16 [4096, 512], P(('ep', 'tp')), may hold values from -6 to 6
- kv_latent: bfloat16 [4096, 256], P(('ep', 'tp')), may hold values from -6 to 6
- rope_key: bfloat16 [4096, 32], P(('ep', 'tp')), may hold values from -240 to 240
- q_gain: float32 [512], replicated, may hold values from 0.1 to 1.9
- kv_gain: float32 [256], replicated, may hold values from 0.1 to 1.9
- w_query: bfloat16 [512, 1024], P(None, 'tp'), may hold values from -0.25 to 0.25
- w_query_rot: bfloat16 [512, 512], P(None, 'tp'), may hold values from -0.25 to 0.25
- w_key: bfloat16 [256, 1024], P(None, 'tp'), may hold values from -0.375 to 0.375
- w_value: bfloat16 [256, 1024], P(None, 'tp'), may hold values from -0.375 to 0.375
- w_mix_out: bfloat16 [1024, 2048], P('tp'), may hold values from -0.1875 to 0.1875
- expert_input: bfloat16 [4096, 2048], P(('ep', 'tp')), may hold values from -6 to 6
- ffn_gain: float32 [2048], replicated, may hold values from 0.1 to 1.9
- expert_ids: int32 [4096, 4], P(('ep', 'tp')), may hold values from 0 to 7, all different within a row; in each aligned block of 128 rows (0 to 127, 128 to 255, ...) at most 96 rows name the same one
- route_weights: float32 [4096, 4], P(('ep', 'tp')), may hold values from 0.2 to 1
- w_gate_exp: bfloat16 [8, 2048, 1024], P('ep', None, 'tp'), may hold values from -0.125 to 0.125
- w_up_exp: bfloat16 [8, 2048, 1024], P('ep', None, 'tp'), may hold values from -0.125 to 0.125
- w_down_exp: bfloat16 [8, 1024, 2048], P('ep', 'tp'), may hold values from -0.1875 to 0.1875
Outputs:
- mixer_out: bfloat16 [4096, 2048], P(('ep', 'tp'))
- expert_out: bfloat16 [4096, 2048], P(('ep', 'tp'))
The draws below stay inside these ranges and needn't reach their ends.
Inputs may be any that keep to these rules, and one draw needn't show every extreme that they name: `expert_ids`: the experts of a row are all different. In the rows of one device (aligned blocks of 128 tokens) no expert is named by more than 96 rows, a bound that some block reaches.
All inputs are finite; a program needn't handle non-finite values.
Results may differ from the reference program's by a relative error of at most 0.012.
The reference program's roundings to bfloat16 on the way count: a program that leaves them out, or rounds other values in their place, can miss the bound.
Values may be sent and summed in bfloat16 or wider, within the bound.
A program may use at most 128 MiB of HBM per device.

```python
import math
import jax
import jax.numpy as jnp
import numpy as np
from jax import lax

D = 2048
HEADS = 16
NOPE = 64
ROPE = 32
VD = 64
Q_RANK = 512
KV_RANK = 256
FF = 1024
TOPK = 4
SEG = 64
TOK_DEV = 128
EXPERTS = 8
TOKENS = 4096
CAP = 96
N_EP = 8
N_TP = 4


def draw_rope_key(key, part):
    drawn = jnp.clip(jax.random.normal(jax.random.fold_in(key, 11), (TOKENS, ROPE), jnp.float32), -6.0, 6.0)
    return drawn.astype(jnp.bfloat16)


def levels(key, dims, split, least, high):
    loudness = 1.0
    for position, blocks in split:
        steps = jax.random.uniform(jax.random.fold_in(jax.random.fold_in(key, 6), position), (blocks,), jnp.float32, least / len(split), high / len(split))
        loudness = loudness * jnp.repeat(jnp.exp(steps), dims[position] // blocks).reshape((-1,) + (1,) * (len(dims) - 1 - position))
    return loudness


def deal_out(key, own, number, rows, number_of, top, bound, skew):
    order = jax.random.permutation(key, number_of)
    packed, ordinary = shares(number_of, rows * top, bound, skew, True), shares(number_of, rows * top, bound, skew, False)
    places = jnp.arange(number_of)

    def named(tallies, offset_by):
        used = int((tallies > 0).sum())
        fixed = max(1, used // 4)
        moved = fixed + (places - fixed + offset_by * (used - fixed)) % max(1, number_of - fixed)
        return jnp.zeros((number_of,), jnp.int32).at[order[jnp.where(places < fixed, places, moved)]].set(jnp.asarray(tallies, jnp.int32))

    tallies = jnp.where(number % 4 == 0, named(packed, number // 4), named(ordinary, number - number // 4 - 1))
    mixed = jax.random.permutation(jax.random.fold_in(own, 3), number_of)
    giver, taker = mixed[0:number_of // 2 * 2:2], mixed[1:number_of // 2 * 2:2]
    slack = jnp.minimum(tallies[giver] - 1, bound - tallies[taker]) // 2
    slack = jnp.where((giver == order[0]) | (taker == order[0]) | (tallies[taker] == 0), 0, jnp.maximum(slack, 0))
    moved = jax.random.randint(jax.random.fold_in(own, 4), (number_of // 2,), 0, 1 << 20) % (slack + 1)
    tallies = tallies.at[giver].add(-moved).at[taker].add(moved)
    members = jnp.searchsorted(jnp.cumsum(tallies), jnp.arange(rows * top), side="right").astype(jnp.int32)
    grid = members.reshape(top, rows).T
    grid = grid[jax.random.permutation(jax.random.fold_in(own, 1), rows)]
    offset_by = jax.random.randint(jax.random.fold_in(own, 2), (rows, 1), 0, top)
    return jnp.take_along_axis(grid, (jnp.arange(top)[None, :] + offset_by) % top, axis=1)


def shares(amount, total, limit, lean, full):
    weights = [(1 << 20) // math.isqrt(rank ** lean) + 1 for rank in range(1, amount + 1)]
    largest = limit if full else min(limit, max(-(-total // amount), total * weights[0] // sum(weights)))
    least = 1 if total - largest >= amount - 1 else 0
    holding, surplus = [largest] + [least] * (amount - 1), total - largest - least * (amount - 1)
    while surplus > 0:
        free = [i for i in range(1, amount) if holding[i] < largest] or [i for i in range(1, amount) if holding[i] < limit]
        whole, budget = sum([weights[i] for i in free]), surplus
        for i in free:
            more = min(limit - holding[i], max(1, budget * weights[i] // whole), surplus)
            holding[i] = holding[i] + more
            surplus = surplus - more
    return np.array(holding)


def noise(key, dims, width, limit, split=(), kind=jnp.bfloat16):
    result = width * jax.random.normal(key, dims, jnp.float32)
    if split:
        result = result * levels(key, dims, split, -0.22, 0.18)
    return jnp.clip(result, -limit, limit).astype(kind)


def setup_inputs(seed: int = 0) -> dict:
    keys = jax.random.split(jax.random.key(seed), 18)
    q_latent = noise(keys[0], (TOKENS, Q_RANK), 1.0, 6.0, ((0, 32),))
    kv_latent = noise(keys[1], (TOKENS, KV_RANK), 1.0, 6.0, ((0, 32),))
    rope_key = draw_rope_key(jax.random.fold_in(keys[17], 71), 0)
    q_gain = jnp.clip(1.0 + 0.18 * jax.random.normal(keys[3], (Q_RANK,), jnp.float32), 0.1, 1.9)
    kv_gain = jnp.clip(1.0 + 0.18 * jax.random.normal(keys[4], (KV_RANK,), jnp.float32), 0.1, 1.9)
    w_query = noise(keys[5], (Q_RANK, HEADS * NOPE), Q_RANK ** -0.5, 0.25, ((1, 4),))
    w_query_rot = noise(keys[6], (Q_RANK, HEADS * ROPE), Q_RANK ** -0.5, 0.25, ((1, 4),))
    w_key = noise(keys[7], (KV_RANK, HEADS * NOPE), KV_RANK ** -0.5, 0.375, ((1, 4),))
    w_value = noise(keys[8], (KV_RANK, HEADS * VD), KV_RANK ** -0.5, 0.375, ((1, 4),))
    w_mix_out = noise(keys[9], (HEADS * VD, D), (HEADS * VD) ** -0.5, 0.1875, ((0, 4),))
    expert_input = noise(keys[10], (TOKENS, D), 1.0, 6.0, ((0, 32),))
    ffn_gain = jnp.clip(1.0 + 0.18 * jax.random.normal(keys[11], (D,), jnp.float32), 0.1, 1.9)
    expert_ids_keys = jax.random.split(jax.random.fold_in(keys[12], 1), TOKENS // TOK_DEV)
    expert_ids_turns = jax.random.permutation(jax.random.fold_in(keys[12], 3), TOKENS // TOK_DEV)
    expert_ids = jax.vmap(lambda own, number: deal_out(jax.random.fold_in(keys[12], 2), own, number, TOK_DEV, EXPERTS, TOPK, CAP, 2))(expert_ids_keys, expert_ids_turns).reshape((TOKENS, TOPK))
    route_weights = jnp.clip(0.2 + 0.8 * jax.random.uniform(keys[13], (TOKENS, TOPK), jnp.float32) ** levels(keys[13], (TOKENS, TOPK), ((0, 32),), -0.2, 0.2), 0.2, 1.0)
    w_gate_exp = noise(keys[14], (EXPERTS, D, FF), D ** -0.5, 0.125, ((0, 8), (2, 4)))
    w_up_exp = noise(keys[15], (EXPERTS, D, FF), D ** -0.5, 0.125, ((0, 8), (2, 4)))
    w_down_exp = noise(keys[16], (EXPERTS, FF, D), FF ** -0.5, 0.1875, ((0, 8), (1, 4)))
    return dict(q_latent=q_latent, kv_latent=kv_latent, rope_key=rope_key, q_gain=q_gain, kv_gain=kv_gain, w_query=w_query, w_query_rot=w_query_rot, w_key=w_key, w_value=w_value, w_mix_out=w_mix_out, expert_input=expert_input, ffn_gain=ffn_gain, expert_ids=expert_ids, route_weights=route_weights, w_gate_exp=w_gate_exp, w_up_exp=w_up_exp, w_down_exp=w_down_exp)


norm_epsilon = 1e-06
rope_base = 10000.0
query_block = 256

def rms_scale(values_in, gain_vec):
    floats = values_in.astype(jnp.float32)
    return floats * lax.rsqrt(lax.optimization_barrier(jnp.mean(floats * floats, axis=-1, keepdims=True)) + norm_epsilon) * gain_vec

def tables(positions):
    half_width = ROPE // 2
    frequency = rope_base ** (-jnp.arange(half_width, dtype=jnp.float32) / half_width)
    angles = positions.astype(jnp.float32)[:, None] * frequency[None, :]
    return (jnp.cos(angles), jnp.sin(angles))

def rotate_pairs(values_in, cosine, sine_table):
    half_width = values_in.shape[-1] // 2
    first, second = (values_in[..., :half_width], values_in[..., half_width:])
    return jnp.concatenate([first * cosine - second * sine_table, first * sine_table + second * cosine], axis=-1)

def mixer(q_latent, kv_latent, rope_key, q_gain, kv_gain, w_query, w_query_rot, w_key, w_value, w_mix_out):
    row_total = q_latent.shape[0]
    positions = jnp.arange(row_total, dtype=jnp.int32)
    cosine, sine_table = tables(positions)
    q_normed = rms_scale(q_latent, q_gain).astype(jnp.bfloat16)
    q_plain = jnp.dot(q_normed, w_query, preferred_element_type=jnp.float32).astype(jnp.bfloat16)
    q_plain = q_plain.reshape(row_total, HEADS, NOPE)
    q_turned = jnp.dot(q_normed, w_query_rot, preferred_element_type=jnp.float32).reshape(row_total, HEADS, ROPE)
    q_turned = rotate_pairs(q_turned, cosine[:, None, :], sine_table[:, None, :]).astype(jnp.bfloat16)
    kv_normed = rms_scale(kv_latent, kv_gain).astype(jnp.bfloat16)
    k_plain = jnp.dot(kv_normed, w_key, preferred_element_type=jnp.float32).astype(jnp.bfloat16)
    k_plain = k_plain.reshape(row_total, HEADS, NOPE).astype(jnp.float32)
    values = jnp.dot(kv_normed, w_value, preferred_element_type=jnp.float32).astype(jnp.bfloat16)
    values = values.reshape(row_total, HEADS, VD).astype(jnp.float32)
    k_turned = rotate_pairs(rope_key.astype(jnp.float32), cosine, sine_table).astype(jnp.bfloat16).astype(jnp.float32)
    segment = positions // SEG
    score_scale = (NOPE + ROPE) ** (-0.5)

    def attend(first_row):
        block_plain = lax.dynamic_slice_in_dim(q_plain, first_row, query_block, 0).astype(jnp.float32)
        block_turned = lax.dynamic_slice_in_dim(q_turned, first_row, query_block, 0).astype(jnp.float32)
        scores = jnp.einsum('qhd,khd->hqk', block_plain, k_plain) + jnp.einsum('qhd,kd->hqk', block_turned, k_turned)
        scores = scores * score_scale
        query_segment = (first_row + jnp.arange(query_block, dtype=jnp.int32)) // SEG
        allowed = segment[None, :] <= query_segment[:, None]
        scores = jnp.where(allowed[None], scores, -jnp.inf)
        row_max = lax.optimization_barrier(jnp.max(scores, axis=-1, keepdims=True))
        weights = jnp.where(allowed[None], jnp.exp(scores - row_max), 0.0)
        weight_sum = lax.optimization_barrier(jnp.sum(weights, axis=-1))
        rounded = weights.astype(jnp.bfloat16).astype(jnp.float32)
        mixed = jnp.einsum('hqk,khd->qhd', rounded, values) / jnp.transpose(weight_sum)[:, :, None]
        return mixed.astype(jnp.bfloat16).reshape(query_block, HEADS * VD)
    starts = jnp.arange(0, row_total, query_block, dtype=jnp.int32)
    attention = lax.map(attend, starts).reshape(row_total, HEADS * VD)
    block_width = HEADS * VD // N_TP
    summed = jnp.zeros((row_total, D), jnp.float32)
    for block_index in range(N_TP):
        columns = attention[:, block_index * block_width:(block_index + 1) * block_width]
        weight_rows = w_mix_out[block_index * block_width:(block_index + 1) * block_width]
        partial_out = jnp.dot(columns, weight_rows, preferred_element_type=jnp.float32).astype(jnp.bfloat16)
        summed = summed + lax.optimization_barrier(partial_out).astype(jnp.float32)
    return summed.astype(jnp.bfloat16)

def experts(expert_input, ffn_gain, expert_ids, route_weights, w_gate_exp, w_up_exp, w_down_exp):
    row_total = expert_input.shape[0]
    groups = N_EP * N_TP
    expert_count = w_gate_exp.shape[0]
    normed = rms_scale(expert_input, ffn_gain).astype(jnp.bfloat16)
    routed = expert_ids.reshape(groups, TOK_DEV * TOPK).astype(jnp.int32)
    onehot = (routed[:, :, None] == jnp.arange(expert_count, dtype=jnp.int32)[None, None, :]).astype(jnp.int32)
    slot_number = lax.optimization_barrier(jnp.sum((jnp.cumsum(onehot, axis=1) - 1) * onehot, axis=-1)).astype(jnp.int32)
    group_index = jnp.arange(groups, dtype=jnp.int32)[:, None]
    slot_place = ((routed * groups + group_index) * CAP + slot_number).reshape(-1).astype(jnp.int32)
    token_index = group_index * TOK_DEV + jnp.arange(TOK_DEV * TOPK, dtype=jnp.int32)[None, :] // TOPK
    token_table = jnp.zeros((expert_count * groups * CAP,), jnp.int32).at[slot_place].set(token_index.reshape(-1).astype(jnp.int32))
    token_table = token_table.reshape(expert_count, groups * CAP)
    block_width = FF // N_TP

    def expert_block(arguments):
        rows_idx, gate_weight, up_weight, down_weight = arguments
        chosen = normed[rows_idx]
        gate_part = jnp.dot(chosen, gate_weight, preferred_element_type=jnp.float32)
        up_part = jnp.dot(chosen, up_weight, preferred_element_type=jnp.float32)
        hidden = (jax.nn.silu(gate_part) * up_part).astype(jnp.bfloat16)
        summed = jnp.zeros((chosen.shape[0], D), jnp.float32)
        for block_index in range(N_TP):
            columns = hidden[:, block_index * block_width:(block_index + 1) * block_width]
            weight_rows = down_weight[block_index * block_width:(block_index + 1) * block_width]
            partial_out = jnp.dot(columns, weight_rows, preferred_element_type=jnp.float32).astype(jnp.bfloat16)
            summed = summed + lax.optimization_barrier(partial_out).astype(jnp.float32)
        return summed.astype(jnp.bfloat16)
    results = lax.map(expert_block, (token_table, w_gate_exp, w_up_exp, w_down_exp))
    all_results = results.reshape(-1, D)
    picked = all_results[slot_place].astype(jnp.float32).reshape(row_total, TOPK, D)
    weighted_sum = lax.optimization_barrier(jnp.sum(picked * route_weights[:, :, None].astype(jnp.float32), axis=1))
    return weighted_sum.astype(jnp.bfloat16)

def reference(q_latent, kv_latent, rope_key, q_gain, kv_gain, w_query, w_query_rot, w_key, w_value, w_mix_out, expert_input, ffn_gain, expert_ids, route_weights, w_gate_exp, w_up_exp, w_down_exp):
    mixer_out = mixer(q_latent, kv_latent, rope_key, q_gain, kv_gain, w_query, w_query_rot, w_key, w_value, w_mix_out)
    expert_out = experts(expert_input, ffn_gain, expert_ids, route_weights, w_gate_exp, w_up_exp, w_down_exp)
    return (mixer_out, expert_out)
```

```python
import functools
import math

import jax
import jax.numpy as jnp
from jax import lax
from jax.experimental import pallas as pl
from jax.experimental.pallas import tpu as pltpu
from jax.sharding import PartitionSpec as P

D = 2048
NOPE = 64
ROPE = 32
VD = 64
TOPK = 4
SEG = 64


norm_epsilon = 1e-06
rope_base = 10000.0
masked_score = -1e30


def rms_scale(values_in, gain_vec):
    floats = values_in.astype(jnp.float32)
    return (
        floats
        * lax.rsqrt(jnp.mean(floats * floats, axis=-1, keepdims=True) + norm_epsilon)
        * gain_vec
    )


def tables(positions):
    half_width = ROPE // 2
    frequency = rope_base ** (-jnp.arange(half_width, dtype=jnp.float32) / half_width)
    angles = positions.astype(jnp.float32)[:, None] * frequency[None, :]
    return (jnp.cos(angles), jnp.sin(angles))


def rotate_pairs(values_in, cosine, sine_table):
    half_width = values_in.shape[-1] // 2
    first, second = (values_in[..., :half_width], values_in[..., half_width:])
    return jnp.concatenate(
        [first * cosine - second * sine_table, first * sine_table + second * cosine], axis=-1
    )


LANES = 128


def pad_heads(weight, heads, width):
    split = weight.reshape(weight.shape[0], heads, width)
    return jnp.pad(split, ((0, 0), (0, 0), (0, LANES - width))).reshape(
        weight.shape[0], heads * LANES
    )


def make_queries(q_rows, q_gain, w_query, w_query_rot, heads, group_rows):
    start = lax.axis_index("ep") * group_rows
    cosine, sine_table = tables(start + jnp.arange(group_rows, dtype=jnp.int32))
    normed = rms_scale(q_rows, q_gain).astype(jnp.bfloat16)
    plain = jnp.dot(normed, w_query, preferred_element_type=jnp.float32).astype(jnp.bfloat16)
    turned = jnp.dot(normed, w_query_rot, preferred_element_type=jnp.float32).reshape(
        group_rows, heads, ROPE
    )
    turned = rotate_pairs(turned, cosine[:, None, :], sine_table[:, None, :]).astype(jnp.bfloat16)
    blank = jnp.zeros((group_rows, heads, LANES - NOPE - ROPE), jnp.bfloat16)
    joined = jnp.concatenate([plain.reshape(group_rows, heads, NOPE), turned, blank], axis=-1)
    return joined.reshape(group_rows, heads * LANES)


def make_keys(kv_rows, kv_gain, w_key, w_value, heads):
    row_count = kv_rows.shape[0]
    rank = w_key.shape[0]
    normed = rms_scale(kv_rows[:, :rank], kv_gain).astype(jnp.bfloat16)
    cosine, sine_table = tables(jnp.arange(row_count, dtype=jnp.int32))
    turned = rotate_pairs(kv_rows[:, rank:].astype(jnp.float32), cosine, sine_table)
    turned = jnp.pad(
        turned.astype(jnp.bfloat16), ((0, 0), (NOPE, LANES - NOPE - ROPE))
    )
    plain = jnp.dot(normed, pad_heads(w_key, heads, NOPE), preferred_element_type=jnp.float32)
    keys = plain.astype(jnp.bfloat16) + jnp.tile(turned, (1, heads))
    raw = jnp.dot(normed, pad_heads(w_value, heads, VD), preferred_element_type=jnp.float32)
    ones = (jnp.arange(heads * LANES, dtype=jnp.int32) % LANES == VD).astype(jnp.bfloat16)
    return keys, raw.astype(jnp.bfloat16) + ones[None, :]


def attention_kernel(heads, chunk, group_ref, q_ref, k_ref, v_ref, o_ref, max_ref, acc_ref):
    step = pl.program_id(0)
    group = group_ref[0]
    rows = q_ref.shape[0]
    keys = k_ref.shape[0]
    log_scale = (NOPE + ROPE) ** (-0.5) * math.log2(math.e)

    @pl.when(step == 0)
    def _():
        max_ref[...] = jnp.full(max_ref.shape, masked_score, jnp.float32)
        acc_ref[...] = jnp.zeros(acc_ref.shape, jnp.float32)

    def work(masked):
        for head in range(heads):
            lanes = slice(head * LANES, (head + 1) * LANES)
            for first in range(0, rows, chunk):
                part = slice(first, first + chunk)
                scores = lax.dot_general(
                    q_ref[part, lanes],
                    k_ref[:, lanes],
                    (((1,), (1,)), ((), ())),
                    preferred_element_type=jnp.float32,
                )
                if masked:
                    row_id = lax.broadcasted_iota(jnp.int32, (chunk, keys), 0) + first
                    col_id = lax.broadcasted_iota(jnp.int32, (chunk, keys), 1)
                    scores = jnp.where(col_id // SEG <= row_id // SEG, scores, masked_score)
                old = max_ref[head, part, :]
                new = jnp.maximum(old, jnp.max(scores, axis=-1, keepdims=True))
                weights = jnp.exp2((scores - new[:, :1]) * log_scale).astype(jnp.bfloat16)
                factor = jnp.exp2((old - new) * log_scale)
                max_ref[head, part, :] = new
                acc_ref[head, part, :] = acc_ref[head, part, :] * factor + jnp.dot(
                    weights, v_ref[:, lanes], preferred_element_type=jnp.float32
                )

    @pl.when(step < group)
    def _():
        work(False)

    @pl.when(step == group)
    def _():
        work(True)

    @pl.when(step == pl.num_programs(0) - 1)
    def _():
        for head in range(heads):
            acc = acc_ref[head]
            o_ref[:, head * VD : (head + 1) * VD] = (
                acc[:, :VD] / acc[:, VD : VD + 1]
            ).astype(jnp.bfloat16)


def attend(queries, keys, values, heads, group_rows):
    group = lax.axis_index("ep").astype(jnp.int32).reshape(1)
    blocks = keys.shape[0] // group_rows
    width = heads * LANES
    chunk = 256 if group_rows % 256 == 0 else group_rows
    return pl.pallas_call(
        functools.partial(attention_kernel, heads, chunk),
        out_shape=jax.ShapeDtypeStruct((group_rows, heads * VD), jnp.bfloat16),
        grid_spec=pltpu.PrefetchScalarGridSpec(
            num_scalar_prefetch=1,
            grid=(blocks,),
            in_specs=[
                pl.BlockSpec((group_rows, width), lambda i, g: (0, 0)),
                pl.BlockSpec((group_rows, width), lambda i, g: (jnp.minimum(i, g[0]), 0)),
                pl.BlockSpec((group_rows, width), lambda i, g: (jnp.minimum(i, g[0]), 0)),
            ],
            out_specs=pl.BlockSpec((group_rows, heads * VD), lambda i, g: (0, 0)),
            scratch_shapes=[
                pltpu.VMEM((heads, group_rows, LANES), jnp.float32),
                pltpu.VMEM((heads, group_rows, LANES), jnp.float32),
            ],
        ),
        compiler_params=pltpu.CompilerParams(
            dimension_semantics=("arbitrary",), vmem_limit_bytes=24 * 1024 * 1024
        ),
        cost_estimate=pl.CostEstimate(
            flops=4 * heads * group_rows * keys.shape[0] * LANES * 2,
            bytes_accessed=4 * keys.shape[0] * width,
            transcendentals=heads * group_rows * keys.shape[0],
        ),
        name="attend",
    )(group, queries, keys, values)


MESH = pl.DeviceIdType.MESH
TILE = 256


def ring_place(index, count):
    side = index % 2
    line = index // 2
    return line + side * (count - 1 - 2 * line)


def ring_index(place, count):
    side = place // (count // 2)
    line = place + side * (count - 1 - 2 * place)
    return 2 * line + side


def remote(src, dst, send, recv, device):
    return pltpu.make_async_remote_copy(
        src_ref=src, dst_ref=dst, send_sem=send, recv_sem=recv, device_id=device, device_id_type=MESH
    )


def expert_kernel(
    count,
    chunks,
    x_ref,
    gain_ref,
    coef_ref,
    gate_ref,
    up_ref,
    down_ref,
    out_ref,
    raw,
    xn,
    wg,
    wu,
    wd,
    hid,
    y,
    from_prev,
    from_next,
    coefs,
    coef_col,
    local_sem,
    coef_send,
    coef_recv,
    fwd_send,
    fwd_recv,
    bwd_send,
    bwd_recv,
    core_send,
    core_recv,
    cross_send,
    cross_recv,
    relay_send,
    relay_recv,
    sum_r_send,
    sum_r_recv,
    sum_l_send,
    sum_l_recv,
):
    rows = x_ref.shape[0]
    half_rows = rows // 2
    half = count // 2
    depth = gate_ref.shape[1]
    ff = gate_ref.shape[2]
    width = out_ref.shape[1] // chunks
    me = lax.axis_index("ep")
    tp = lax.axis_index("tp")
    place = ring_place(me, count)
    nxt = (ring_index((place + 1) % count, count), tp)
    prv = (ring_index((place + count - 1) % count, count), tp)
    core_peer = (me, tp + 1 - 2 * (tp % 2))
    cross_peer = (me, (tp + 2) % 4)

    barrier = pltpu.get_barrier_semaphore()
    for step in range(1, count):
        pl.semaphore_signal(
            barrier,
            inc=1,
            device_id=(ring_index((place + step) % count, count), tp),
            device_id_type=MESH,
        )
    for peer in (core_peer, cross_peer):
        pl.semaphore_signal(barrier, inc=1, device_id=peer, device_id_type=MESH)
    pl.semaphore_wait(barrier, count + 1)

    sent = []

    def go(copy):
        copy.start()
        sent.append(copy)
        return copy

    def half_of(h):
        return pl.ds(h * half_rows, half_rows)

    def forward(step, h):
        src = x_ref.at[half_of(h)] if step == 1 else raw.at[step - 1, half_of(h)]
        return remote(
            src, raw.at[step, half_of(h)], fwd_send.at[step, h], fwd_recv.at[step, h], nxt
        )

    def backward(step, h):
        src = x_ref.at[half_of(h)] if step == 1 else raw.at[count - step + 1, half_of(h)]
        return remote(
            src, raw.at[count - step, half_of(h)], bwd_send.at[step, h], bwd_recv.at[step, h], prv
        )

    def piece(i, slot):
        if i < 4:
            ref = (wg, wu)[i // 2]
            return ref.at[slot, pl.ds((i % 2) * (depth // 2), depth // 2)]
        return wd.at[i - 4, pl.ds(slot * ff, ff)]

    def own_piece(i):
        if i < 4:
            ref = (gate_ref, up_ref)[i // 2]
            return ref.at[0, pl.ds((i % 2) * (depth // 2), depth // 2)]
        return down_ref.at[0, :, pl.ds((i - 4) * width, width)]

    pieces = 4 + chunks
    ring = {}
    for h in range(2):
        ring["f", 1, h] = go(forward(1, h))
        ring["b", 1, h] = go(backward(1, h))
    to_coefs = []
    for step in range(1, count):
        to_coefs.append(
            go(
                remote(
                    coef_ref,
                    coefs.at[step],
                    coef_send.at[step],
                    coef_recv.at[step],
                    (ring_index((place + step) % count, count), tp),
                )
            )
        )
    local, to_core, to_cross, relay = [], [], [], []
    for i in range(pieces):
        to_cross.append(
            go(remote(own_piece(i), piece(i, 2), cross_send.at[i], cross_recv.at[i], cross_peer))
        )
        to_core.append(
            go(remote(own_piece(i), piece(i, 1), core_send.at[i], core_recv.at[i], core_peer))
        )
        copy = pltpu.make_async_copy(own_piece(i), piece(i, 0), local_sem.at[i])
        copy.start()
        local.append(copy)

    def pass_on(i):
        to_cross[i].wait_recv()
        relay.append(
            go(remote(piece(i, 2), piece(i, 3), relay_send.at[i], relay_recv.at[i], core_peer))
        )

    def norm(slot):
        source = x_ref if slot == 0 else raw.at[slot]
        floats = source[...].astype(jnp.float32)
        scale = lax.rsqrt(jnp.mean(floats * floats, axis=-1, keepdims=True) + norm_epsilon)
        xn[slot * rows : (slot + 1) * rows, :] = (floats * scale * gain_ref[...]).astype(
            jnp.bfloat16
        )

    def coefficient(slot):
        source = coef_ref if slot == 0 else coefs.at[slot]
        line = jnp.broadcast_to(source[pl.ds(me, 1), :], (rows, rows))
        row_id = lax.broadcasted_iota(jnp.int32, (rows, rows), 0)
        col_id = lax.broadcasted_iota(jnp.int32, (rows, rows), 1)
        coef_col[slot * rows : (slot + 1) * rows, :] = jnp.sum(
            jnp.where(row_id == col_id, line, 0.0), axis=-1, keepdims=True
        )

    norm(0)
    coefficient(0)
    for step in range(1, half):
        for h in range(2):
            ring["f", step, h].wait_recv()
            if step + 1 < half or h == 0:
                ring["f", step + 1, h] = go(forward(step + 1, h))
            ring["b", step, h].wait_recv()
            if step + 1 < half or h == 1:
                ring["b", step + 1, h] = go(backward(step + 1, h))
        norm(step)
        norm(count - step)
        if step == 1:
            for copy in to_coefs:
                copy.wait_recv()
            for slot in range(1, count):
                coefficient(slot)
        if step < 4:
            pass_on(step - 1)
    ring["f", half, 0].wait_recv()
    ring["b", half, 1].wait_recv()
    norm(half)
    while len(relay) < 3:
        pass_on(len(relay))

    total_rows = count * rows

    def hidden(first, last):
        @pl.loop(first, last)
        def _(slot):
            @pl.loop(0, total_rows // TILE)
            def _(tile):
                part = pl.ds(pl.multiple_of(tile * TILE, TILE), TILE)
                tokens = xn[part, :]
                gate = jnp.dot(tokens, wg[slot], preferred_element_type=jnp.float32)
                up = jnp.dot(tokens, wu[slot], preferred_element_type=jnp.float32)
                hid[part, pl.ds(pl.multiple_of(slot * ff, ff), ff)] = (
                    gate * jax.nn.sigmoid(gate) * up
                ).astype(jnp.bfloat16)

    for i in range(4):
        local[i].wait()
        to_core[i].wait_recv()
    hidden(0, 2)
    pass_on(3)
    for i in range(4):
        relay[i].wait_recv()
    hidden(2, 4)

    def down(c):
        pass_on(4 + c)
        local[4 + c].wait()
        to_core[4 + c].wait_recv()
        relay[4 + c].wait_recv()

        @pl.loop(0, total_rows // TILE)
        def _(tile):
            part = pl.ds(pl.multiple_of(tile * TILE, TILE), TILE)
            acc = jnp.dot(hid[part, :], wd[c], preferred_element_type=jnp.float32)
            y[c, part, :] = (acc * coef_col[part, :]).astype(jnp.bfloat16)

    def block(slot, h=None):
        if h is None:
            return pl.ds(slot * rows, rows)
        return pl.ds(slot * rows + h * half_rows, half_rows)

    sums = {}

    def sum_start(c):
        sums["r", c, 0] = go(
            remote(
                y.at[c, block(half, 0)],
                from_prev.at[c, 0, half_of(0)],
                sum_r_send.at[c, 0],
                sum_r_recv.at[c, 0],
                nxt,
            )
        )
        sums["l", c, 0] = go(
            remote(
                y.at[c, block(half, 1)],
                from_next.at[c, 0, half_of(1)],
                sum_l_send.at[c, 0],
                sum_l_recv.at[c, 0],
                prv,
            )
        )

    def add(target, source):
        target[...] = (target[...].astype(jnp.float32) + source[...].astype(jnp.float32)).astype(
            jnp.bfloat16
        )

    def sum_step(c, k):
        sums["r", c, k - 1].wait_recv()
        if k == 1:
            add(y.at[c, block(half + k, 0)], from_prev.at[c, 0, half_of(0)])
        else:
            add(y.at[c, block(half + k)], from_prev.at[c, k - 1])
        sums["r", c, k] = go(
            remote(
                y.at[c, block(half + k)],
                from_prev.at[c, k],
                sum_r_send.at[c, k],
                sum_r_recv.at[c, k],
                nxt,
            )
        )
        sums["l", c, k - 1].wait_recv()
        if k == 1:
            add(y.at[c, block(half - k, 1)], from_next.at[c, 0, half_of(1)])
        else:
            add(y.at[c, block(half - k)], from_next.at[c, k - 1])
        sums["l", c, k] = go(
            remote(
                y.at[c, block(half - k)],
                from_next.at[c, k],
                sum_l_send.at[c, k],
                sum_l_recv.at[c, k],
                prv,
            )
        )

    def sum_end(c):
        sums["r", c, half - 1].wait_recv()
        sums["l", c, half - 1].wait_recv()
        out_ref[:, c * width : (c + 1) * width] = (
            y[c, block(0), :].astype(jnp.float32)
            + from_prev[c, half - 1].astype(jnp.float32)
            + from_next[c, half - 1].astype(jnp.float32)
        ).astype(jnp.bfloat16)

    for tick in range(chunks + half):
        for c in range(chunks):
            k = tick - c
            if 1 <= k < half:
                sum_step(c, k)
            elif k == half:
                sum_end(c)
        if tick < chunks:
            down(tick)
            sum_start(tick)
    for copy in sent:
        copy.wait_send()


def run_experts(expert_input, ffn_gain, coef, gate, up, down, count, chunks):
    rows, depth = expert_input.shape
    ff = gate.shape[2]
    half = count // 2
    width = depth // chunks
    pieces = 4 + chunks
    bf16 = jnp.bfloat16
    dma = pltpu.SemaphoreType.DMA
    vmem = pl.BlockSpec(memory_space=pltpu.VMEM)
    hbm = pl.BlockSpec(memory_space=pl.ANY)
    return pl.pallas_call(
        functools.partial(expert_kernel, count, chunks),
        out_shape=jax.ShapeDtypeStruct((rows, depth), bf16),
        in_specs=[vmem, vmem, vmem, hbm, hbm, hbm],
        out_specs=vmem,
        scratch_shapes=[
            pltpu.VMEM((count, rows, depth), bf16),
            pltpu.VMEM((count * rows, depth), bf16),
            pltpu.VMEM((4, depth, ff), bf16),
            pltpu.VMEM((4, depth, ff), bf16),
            pltpu.VMEM((chunks, 4 * ff, width), bf16),
            pltpu.VMEM((count * rows, 4 * ff), bf16),
            pltpu.VMEM((chunks, count * rows, width), bf16),
            pltpu.VMEM((chunks, half, rows, width), bf16),
            pltpu.VMEM((chunks, half, rows, width), bf16),
            pltpu.VMEM((count, count, rows), jnp.float32),
            pltpu.VMEM((count * rows, 1), jnp.float32),
            dma((pieces,)),
            dma((count,)),
            dma((count,)),
            dma((half + 1, 2)),
            dma((half + 1, 2)),
            dma((half + 1, 2)),
            dma((half + 1, 2)),
            dma((pieces,)),
            dma((pieces,)),
            dma((pieces,)),
            dma((pieces,)),
            dma((pieces,)),
            dma((pieces,)),
            dma((chunks, half)),
            dma((chunks, half)),
            dma((chunks, half)),
            dma((chunks, half)),
        ],
        compiler_params=pltpu.CompilerParams(
            collective_id=0, has_side_effects=True, vmem_limit_bytes=60 * 1024 * 1024
        ),
        cost_estimate=pl.CostEstimate(
            flops=6 * count * rows * depth * 4 * ff,
            bytes_accessed=12 * depth * ff * 2,
            transcendentals=count * rows * 4 * ff,
        ),
        name="experts",
    )(expert_input, ffn_gain.reshape(1, -1), coef, gate, up, down)


def on_device_plain(
    q_latent,
    kv_latent,
    rope_key,
    q_gain,
    kv_gain,
    w_query,
    w_query_rot,
    w_key,
    w_value,
    w_mix_out,
    expert_input,
    ffn_gain,
    expert_ids,
    route_weights,
    w_gate_exp,
    w_up_exp,
    w_down_exp,
):
    tok_rows = q_latent.shape[0]
    tp_count = lax.axis_size("tp")
    expert_count = lax.axis_size("ep")
    slot_count = 3 * tok_rows * TOPK // (2 * expert_count)
    group_rows = tp_count * tok_rows
    heads_here = w_key.shape[1] // NOPE

    gate_all = lax.all_gather(w_gate_exp[0], "tp", axis=0)
    up_all = lax.all_gather(w_up_exp[0], "tp", axis=0)
    down_all = lax.all_gather(w_down_exp[0], "tp", axis=0)

    normed = rms_scale(expert_input, ffn_gain).astype(jnp.bfloat16)
    routed = expert_ids.reshape(-1)
    onehot = (routed[:, None] == jnp.arange(expert_count, dtype=jnp.int32)[None, :]).astype(
        jnp.int32
    )
    slot_number = jnp.sum((jnp.cumsum(onehot, axis=0) - 1) * onehot, axis=-1)
    slot_place = (routed * slot_count + slot_number).reshape(tok_rows, TOPK)
    slot_line = jnp.arange(expert_count * slot_count, dtype=jnp.int32)
    picks = [
        (slot_place[:, route_rank][:, None] == slot_line[None, :]).astype(jnp.bfloat16)
        for route_rank in range(TOPK)
    ]
    dispatch = picks[0]
    for route_rank in range(1, TOPK):
        dispatch = dispatch + picks[route_rank]
    outgoing = lax.dot_general(
        dispatch, normed, (((0,), (0,)), ((), ())), preferred_element_type=jnp.float32
    ).astype(jnp.bfloat16)
    arrived = lax.all_to_all(
        outgoing.reshape(expert_count, slot_count, D), "ep", split_axis=0, concat_axis=0, tiled=True
    )
    rows = arrived.reshape(expert_count * slot_count, D)

    own_rows = jnp.concatenate([kv_latent, rope_key], axis=1)
    ep_rows = lax.all_gather(own_rows, "ep", axis=0, tiled=True)
    column_count = own_rows.shape[1]
    piece_width = column_count // 3 if column_count % 3 == 0 else column_count
    pieces = [
        lax.all_gather(ep_rows[:, first : first + piece_width], "tp", axis=0)
        for first in range(0, column_count, piece_width)
    ]
    kv_rows = (
        jnp.concatenate(pieces, axis=2)
        .reshape(tp_count, expert_count, tok_rows, column_count)
        .transpose(1, 0, 2, 3)
        .reshape(expert_count * group_rows, column_count)
    )
    q_rows = lax.all_gather(q_latent, "tp", axis=0, tiled=True)
    queries = make_queries(q_rows, q_gain, w_query, w_query_rot, heads_here, group_rows)
    keys, values = make_keys(kv_rows, kv_gain, w_key, w_value, heads_here)
    attention = attend(queries, keys, values, heads_here, group_rows)

    total = jnp.zeros((rows.shape[0], D), jnp.float32)
    for block in range(tp_count):
        gate_part = jnp.dot(rows, gate_all[block], preferred_element_type=jnp.float32)
        up_part = jnp.dot(rows, up_all[block], preferred_element_type=jnp.float32)
        hidden = (jax.nn.silu(gate_part) * up_part).astype(jnp.bfloat16)
        part = jnp.dot(hidden, down_all[block], preferred_element_type=jnp.float32)
        total = total + part.astype(jnp.bfloat16).astype(jnp.float32)
    summed = total.astype(jnp.bfloat16)
    results = lax.all_to_all(
        summed.reshape(expert_count, slot_count, D), "ep", split_axis=0, concat_axis=0, tiled=True
    ).reshape(expert_count * slot_count, D)

    partial_out = jnp.dot(attention, w_mix_out, preferred_element_type=jnp.float32).astype(
        jnp.bfloat16
    )
    mixer_out = lax.psum_scatter(partial_out, "tp", scatter_dimension=0, tiled=True)

    fetched = jnp.dot(
        jnp.concatenate(picks, axis=0), results, preferred_element_type=jnp.float32
    ).astype(jnp.bfloat16)
    combined = jnp.zeros((tok_rows, D), jnp.float32)
    for route_rank in range(TOPK):
        piece = fetched[route_rank * tok_rows : (route_rank + 1) * tok_rows].astype(jnp.float32)
        combined = combined + route_weights[:, route_rank : route_rank + 1] * piece
    return (mixer_out, combined.astype(jnp.bfloat16))


def coefficients(expert_ids, route_weights, expert_count):
    experts = jnp.arange(expert_count, dtype=jnp.int32)
    named = expert_ids.T[:, None, :] == experts[None, :, None]
    return jnp.sum(jnp.where(named, route_weights.T[:, None, :], 0.0), axis=0)


def attention_branch(
    q_latent, kv_latent, rope_key, q_gain, kv_gain, w_query, w_query_rot, w_key, w_value, w_mix_out
):
    tok_rows = q_latent.shape[0]
    tp_count = lax.axis_size("tp")
    expert_count = lax.axis_size("ep")
    group_rows = tp_count * tok_rows
    heads_here = w_key.shape[1] // NOPE
    own_rows = jnp.concatenate([kv_latent, rope_key], axis=1)
    tp_rows = lax.all_gather(own_rows, "tp", axis=0, tiled=True)
    kv_rows = lax.all_gather(tp_rows, "ep", axis=0, tiled=True)
    q_rows = lax.all_gather(q_latent, "tp", axis=0, tiled=True)
    queries = make_queries(q_rows, q_gain, w_query, w_query_rot, heads_here, group_rows)
    keys, values = make_keys(kv_rows, kv_gain, w_key, w_value, heads_here)
    attention = attend(queries, keys, values, heads_here, group_rows)
    partial_out = jnp.dot(attention, w_mix_out, preferred_element_type=jnp.float32).astype(
        jnp.bfloat16
    )
    return lax.psum_scatter(partial_out, "tp", scatter_dimension=0, tiled=True)


def on_device_fused(

    q_latent,
    kv_latent,
    rope_key,
    q_gain,
    kv_gain,
    w_query,
    w_query_rot,
    w_key,
    w_value,
    w_mix_out,
    expert_input,
    ffn_gain,
    expert_ids,
    route_weights,
    w_gate_exp,
    w_up_exp,
    w_down_exp,
):
    expert_count = lax.axis_size("ep")
    coef = coefficients(expert_ids, route_weights, expert_count)
    expert_out = run_experts(
        expert_input, ffn_gain, coef, w_gate_exp, w_up_exp, w_down_exp, expert_count, 4
    )
    mixer_out = attention_branch(
        q_latent, kv_latent, rope_key, q_gain, kv_gain, w_query, w_query_rot, w_key, w_value, w_mix_out
    )
    return (mixer_out, expert_out)


def fits(mesh):
    ep, tp = mesh.shape["ep"], mesh.shape["tp"]
    return tp == 4 and ep % 2 == 0 and 4 <= ep <= 8


def solution(mesh):
    return jax.shard_map(
        on_device_fused if fits(mesh) else on_device_plain,
        mesh=mesh,
        in_specs=(
            P(("ep", "tp"), None),
            P(("ep", "tp"), None),
            P(("ep", "tp"), None),
            P(),
            P(),
            P(None, "tp"),
            P(None, "tp"),
            P(None, "tp"),
            P(None, "tp"),
            P("tp", None),
            P(("ep", "tp"), None),
            P(),
            P(("ep", "tp"), None),
            P(("ep", "tp"), None),
            P("ep", None, "tp"),
            P("ep", None, "tp"),
            P("ep", "tp", None),
        ),
        out_specs=(P(("ep", "tp"), None), P(("ep", "tp"), None)),
        check_vma=False,
    )
```

```python
import functools
import math

import jax
import jax.numpy as jnp
from jax import lax
from jax.experimental import pallas as pl
from jax.experimental.pallas import tpu as pltpu
from jax.sharding import PartitionSpec as P

D = 2048
NOPE = 64
ROPE = 32
VD = 64
TOPK = 4
SEG = 64


norm_epsilon = 1e-06
rope_base = 10000.0
masked_score = -1e30


def rms_scale(values_in, gain_vec):
    floats = values_in.astype(jnp.float32)
    return (
        floats
        * lax.rsqrt(jnp.mean(floats * floats, axis=-1, keepdims=True) + norm_epsilon)
        * gain_vec
    )


def tables(positions):
    half_width = ROPE // 2
    frequency = rope_base ** (-jnp.arange(half_width, dtype=jnp.float32) / half_width)
    angles = positions.astype(jnp.float32)[:, None] * frequency[None, :]
    return (jnp.cos(angles), jnp.sin(angles))


def rotate_pairs(values_in, cosine, sine_table):
    half_width = values_in.shape[-1] // 2
    first, second = (values_in[..., :half_width], values_in[..., half_width:])
    return jnp.concatenate(
        [first * cosine - second * sine_table, first * sine_table + second * cosine], axis=-1
    )


LANES = 128


def pad_heads(weight, heads, width):
    split = weight.reshape(weight.shape[0], heads, width)
    return jnp.pad(split, ((0, 0), (0, 0), (0, LANES - width))).reshape(
        weight.shape[0], heads * LANES
    )


def make_queries(q_rows, q_gain, w_query, w_query_rot, heads, group_rows):
    start = lax.axis_index("ep") * group_rows
    cosine, sine_table = tables(start + jnp.arange(group_rows, dtype=jnp.int32))
    normed = rms_scale(q_rows, q_gain).astype(jnp.bfloat16)
    plain = jnp.dot(normed, w_query, preferred_element_type=jnp.float32).astype(jnp.bfloat16)
    turned = jnp.dot(normed, w_query_rot, preferred_element_type=jnp.float32).reshape(
        group_rows, heads, ROPE
    )
    turned = rotate_pairs(turned, cosine[:, None, :], sine_table[:, None, :]).astype(jnp.bfloat16)
    blank = jnp.zeros((group_rows, heads, LANES - NOPE - ROPE), jnp.bfloat16)
    joined = jnp.concatenate([plain.reshape(group_rows, heads, NOPE), turned, blank], axis=-1)
    return joined.reshape(group_rows, heads * LANES)


def make_keys(kv_rows, kv_gain, w_key, w_value, heads):
    row_count = kv_rows.shape[0]
    rank = w_key.shape[0]
    normed = rms_scale(kv_rows[:, :rank], kv_gain).astype(jnp.bfloat16)
    cosine, sine_table = tables(jnp.arange(row_count, dtype=jnp.int32))
    turned = rotate_pairs(kv_rows[:, rank:].astype(jnp.float32), cosine, sine_table)
    turned = jnp.pad(
        turned.astype(jnp.bfloat16), ((0, 0), (NOPE, LANES - NOPE - ROPE))
    )
    plain = jnp.dot(normed, pad_heads(w_key, heads, NOPE), preferred_element_type=jnp.float32)
    keys = plain.astype(jnp.bfloat16) + jnp.tile(turned, (1, heads))
    raw = jnp.dot(normed, pad_heads(w_value, heads, VD), preferred_element_type=jnp.float32)
    ones = (jnp.arange(heads * LANES, dtype=jnp.int32) % LANES == VD).astype(jnp.bfloat16)
    return keys, raw.astype(jnp.bfloat16) + ones[None, :]


def attention_kernel(heads, chunk, group_ref, q_ref, k_ref, v_ref, o_ref, max_ref, acc_ref):
    step = pl.program_id(0)
    group = group_ref[0]
    rows = q_ref.shape[0]
    keys = k_ref.shape[0]
    log_scale = (NOPE + ROPE) ** (-0.5) * math.log2(math.e)

    @pl.when(step == 0)
    def _():
        max_ref[...] = jnp.full(max_ref.shape, masked_score, jnp.float32)
        acc_ref[...] = jnp.zeros(acc_ref.shape, jnp.float32)

    def work(masked):
        for head in range(heads):
            lanes = slice(head * LANES, (head + 1) * LANES)
            for first in range(0, rows, chunk):
                part = slice(first, first + chunk)
                scores = lax.dot_general(
                    q_ref[part, lanes],
                    k_ref[:, lanes],
                    (((1,), (1,)), ((), ())),
                    preferred_element_type=jnp.float32,
                )
                if masked:
                    row_id = lax.broadcasted_iota(jnp.int32, (chunk, keys), 0) + first
                    col_id = lax.broadcasted_iota(jnp.int32, (chunk, keys), 1)
                    scores = jnp.where(col_id // SEG <= row_id // SEG, scores, masked_score)
                old = max_ref[head, part, :]
                new = jnp.maximum(old, jnp.max(scores, axis=-1, keepdims=True))
                weights = jnp.exp2((scores - new[:, :1]) * log_scale).astype(jnp.bfloat16)
                factor = jnp.exp2((old - new) * log_scale)
                max_ref[head, part, :] = new
                acc_ref[head, part, :] = acc_ref[head, part, :] * factor + jnp.dot(
                    weights, v_ref[:, lanes], preferred_element_type=jnp.float32
                )

    @pl.when(step < group)
    def _():
        work(False)

    @pl.when(step == group)
    def _():
        work(True)

    @pl.when(step == pl.num_programs(0) - 1)
    def _():
        for head in range(heads):
            acc = acc_ref[head]
            o_ref[:, head * VD : (head + 1) * VD] = (
                acc[:, :VD] / acc[:, VD : VD + 1]
            ).astype(jnp.bfloat16)


def attend(queries, keys, values, heads, group_rows):
    group = lax.axis_index("ep").astype(jnp.int32).reshape(1)
    blocks = keys.shape[0] // group_rows
    width = heads * LANES
    chunk = 256 if group_rows % 256 == 0 else group_rows
    return pl.pallas_call(
        functools.partial(attention_kernel, heads, chunk),
        out_shape=jax.ShapeDtypeStruct((group_rows, heads * VD), jnp.bfloat16),
        grid_spec=pltpu.PrefetchScalarGridSpec(
            num_scalar_prefetch=1,
            grid=(blocks,),
            in_specs=[
                pl.BlockSpec((group_rows, width), lambda i, g: (0, 0)),
                pl.BlockSpec((group_rows, width), lambda i, g: (jnp.minimum(i, g[0]), 0)),
                pl.BlockSpec((group_rows, width), lambda i, g: (jnp.minimum(i, g[0]), 0)),
            ],
            out_specs=pl.BlockSpec((group_rows, heads * VD), lambda i, g: (0, 0)),
            scratch_shapes=[
                pltpu.VMEM((heads, group_rows, LANES), jnp.float32),
                pltpu.VMEM((heads, group_rows, LANES), jnp.float32),
            ],
        ),
        compiler_params=pltpu.CompilerParams(
            dimension_semantics=("arbitrary",), vmem_limit_bytes=24 * 1024 * 1024
        ),
        cost_estimate=pl.CostEstimate(
            flops=4 * heads * group_rows * keys.shape[0] * LANES * 2,
            bytes_accessed=4 * keys.shape[0] * width,
            transcendentals=heads * group_rows * keys.shape[0],
        ),
        name="attend",
    )(group, queries, keys, values)


def on_device_plain(
    q_latent,
    kv_latent,
    rope_key,
    q_gain,
    kv_gain,
    w_query,
    w_query_rot,
    w_key,
    w_value,
    w_mix_out,
    expert_input,
    ffn_gain,
    expert_ids,
    route_weights,
    w_gate_exp,
    w_up_exp,
    w_down_exp,
):
    tok_rows = q_latent.shape[0]
    tp_count = lax.axis_size("tp")
    expert_count = lax.axis_size("ep")
    slot_count = 3 * tok_rows * TOPK // (2 * expert_count)
    group_rows = tp_count * tok_rows
    heads_here = w_key.shape[1] // NOPE

    gate_all = lax.all_gather(w_gate_exp[0], "tp", axis=0)
    up_all = lax.all_gather(w_up_exp[0], "tp", axis=0)
    down_all = lax.all_gather(w_down_exp[0], "tp", axis=0)

    normed = rms_scale(expert_input, ffn_gain).astype(jnp.bfloat16)
    routed = expert_ids.reshape(-1)
    onehot = (routed[:, None] == jnp.arange(expert_count, dtype=jnp.int32)[None, :]).astype(
        jnp.int32
    )
    slot_number = jnp.sum((jnp.cumsum(onehot, axis=0) - 1) * onehot, axis=-1)
    slot_place = (routed * slot_count + slot_number).reshape(tok_rows, TOPK)
    slot_line = jnp.arange(expert_count * slot_count, dtype=jnp.int32)
    picks = [
        (slot_place[:, route_rank][:, None] == slot_line[None, :]).astype(jnp.bfloat16)
        for route_rank in range(TOPK)
    ]
    dispatch = picks[0]
    for route_rank in range(1, TOPK):
        dispatch = dispatch + picks[route_rank]
    outgoing = lax.dot_general(
        dispatch, normed, (((0,), (0,)), ((), ())), preferred_element_type=jnp.float32
    ).astype(jnp.bfloat16)
    arrived = lax.all_to_all(
        outgoing.reshape(expert_count, slot_count, D), "ep", split_axis=0, concat_axis=0, tiled=True
    )
    rows = arrived.reshape(expert_count * slot_count, D)

    own_rows = jnp.concatenate([kv_latent, rope_key], axis=1)
    ep_rows = lax.all_gather(own_rows, "ep", axis=0, tiled=True)
    column_count = own_rows.shape[1]
    piece_width = column_count // 3 if column_count % 3 == 0 else column_count
    pieces = [
        lax.all_gather(ep_rows[:, first : first + piece_width], "tp", axis=0)
        for first in range(0, column_count, piece_width)
    ]
    kv_rows = (
        jnp.concatenate(pieces, axis=2)
        .reshape(tp_count, expert_count, tok_rows, column_count)
        .transpose(1, 0, 2, 3)
        .reshape(expert_count * group_rows, column_count)
    )
    q_rows = lax.all_gather(q_latent, "tp", axis=0, tiled=True)
    queries = make_queries(q_rows, q_gain, w_query, w_query_rot, heads_here, group_rows)
    keys, values = make_keys(kv_rows, kv_gain, w_key, w_value, heads_here)
    attention = attend(queries, keys, values, heads_here, group_rows)

    total = jnp.zeros((rows.shape[0], D), jnp.float32)
    for block in range(tp_count):
        gate_part = jnp.dot(rows, gate_all[block], preferred_element_type=jnp.float32)
        up_part = jnp.dot(rows, up_all[block], preferred_element_type=jnp.float32)
        hidden = (jax.nn.silu(gate_part) * up_part).astype(jnp.bfloat16)
        part = jnp.dot(hidden, down_all[block], preferred_element_type=jnp.float32)
        total = total + part.astype(jnp.bfloat16).astype(jnp.float32)
    summed = total.astype(jnp.bfloat16)
    results = lax.all_to_all(
        summed.reshape(expert_count, slot_count, D), "ep", split_axis=0, concat_axis=0, tiled=True
    ).reshape(expert_count * slot_count, D)

    partial_out = jnp.dot(attention, w_mix_out, preferred_element_type=jnp.float32).astype(
        jnp.bfloat16
    )
    mixer_out = lax.psum_scatter(partial_out, "tp", scatter_dimension=0, tiled=True)

    fetched = jnp.dot(
        jnp.concatenate(picks, axis=0), results, preferred_element_type=jnp.float32
    ).astype(jnp.bfloat16)
    combined = jnp.zeros((tok_rows, D), jnp.float32)
    for route_rank in range(TOPK):
        piece = fetched[route_rank * tok_rows : (route_rank + 1) * tok_rows].astype(jnp.float32)
        combined = combined + route_weights[:, route_rank : route_rank + 1] * piece
    return (mixer_out, combined.astype(jnp.bfloat16))


MESH = pl.DeviceIdType.MESH


def ring_place(index, count):
    side = index % 2
    line = index // 2
    return line + side * (count - 1 - 2 * line)


def ring_index(place, count):
    side = place // (count // 2)
    line = place + side * (count - 1 - 2 * place)
    return 2 * line + side


def remote(src, dst, send, recv, device):
    return pltpu.make_async_remote_copy(
        src_ref=src, dst_ref=dst, send_sem=send, recv_sem=recv, device_id=device, device_id_type=MESH
    )


def layer_kernel(
    count,
    chunks,
    q_ref,
    kv_ref,
    rope_ref,
    q_gain_ref,
    kv_gain_ref,
    w_query_ref,
    w_rot_ref,
    w_key_ref,
    w_value_ref,
    w_mix_ref,
    cos_ref,
    sin_ref,
    x_ref,
    gain_ref,
    coef_ref,
    gate_ref,
    up_ref,
    down_ref,
    mix_out_ref,
    out_ref,
    q_all,
    wq_cat,
    queries,
    kv_all,
    w_kv,
    kv_now,
    row_max,
    row_acc,
    attended,
    mixed,
    from_core,
    from_cross,
    raw,
    xn,
    wgu,
    wd,
    hid,
    y,
    from_prev,
    from_next,
    coefs,
    coef_col,
    q_send,
    q_recv,
    kvx_sem,
    kvf_send,
    kvf_recv,
    kvb_send,
    kvb_recv,
    kvc_send,
    kvc_recv,
    mix_send,
    mix_recv,
    local_sem,
    coef_send,
    coef_recv,
    fwd_send,
    fwd_recv,
    bwd_send,
    bwd_recv,
    core_send,
    core_recv,
    cross_send,
    cross_recv,
    relay_send,
    relay_recv,
    sum_r_send,
    sum_r_recv,
    sum_l_send,
    sum_l_recv,
):
    bf16, f32 = jnp.bfloat16, jnp.float32
    rows = x_ref.shape[0]
    half_rows = rows // 2
    half = count // 2
    ff = gate_ref.shape[2]
    fh = ff // 2
    width = out_ref.shape[1] // chunks
    group_rows = 4 * rows
    heads = w_key_ref.shape[1] // NOPE
    rank = kv_ref.shape[1]
    head_lanes = heads * LANES
    me = lax.axis_index("ep")
    tp = lax.axis_index("tp")
    place = ring_place(me, count)
    nxt = (ring_index((place + 1) % count, count), tp)
    prv = (ring_index((place + count - 1) % count, count), tp)
    core_peer = (me, tp + 1 - 2 * (tp % 2))
    cross_peer = (me, (tp + 2) % 4)
    diag_peer = (me, 3 - tp)

    barrier = pltpu.get_barrier_semaphore()
    for step in range(1, count):
        pl.semaphore_signal(
            barrier,
            inc=1,
            device_id=(ring_index((place + step) % count, count), tp),
            device_id_type=MESH,
        )
    for peer in (core_peer, cross_peer, diag_peer):
        pl.semaphore_signal(barrier, inc=1, device_id=peer, device_id_type=MESH)

    def rows_of(index):
        return pl.ds(pl.multiple_of(index * rows, rows), rows)

    own_rows, cross_rows = rows_of(tp), rows_of((tp + 2) % 4)

    def scaled(ref, gain):
        floats = ref[...].astype(f32)
        scale = lax.rsqrt(jnp.mean(floats * floats, axis=-1, keepdims=True) + norm_epsilon)
        return (floats * scale * gain[...]).astype(bf16)

    turn_row = lax.broadcasted_iota(jnp.int32, (ROPE, LANES), 0)
    turn_col = lax.broadcasted_iota(jnp.int32, (ROPE, LANES), 1) - NOPE
    straight = (turn_row == turn_col).astype(f32).astype(bf16)
    swapped = (
        ((turn_row == turn_col + ROPE // 2) & (turn_col < ROPE // 2))
        | ((turn_row == turn_col - ROPE // 2) & (turn_col >= ROPE // 2))
    )
    swapped = jnp.where(swapped, 1.0, 0.0).astype(bf16)
    rope = rope_ref[...]
    turned = (
        jnp.dot(rope, straight, preferred_element_type=f32) * cos_ref[own_rows, :]
        + jnp.dot(rope, swapped, preferred_element_type=f32) * sin_ref[own_rows, :]
    )
    lane = lax.broadcasted_iota(jnp.int32, (rows, LANES), 1)
    kv_all[0, own_rows, 0:rank] = scaled(kv_ref, kv_gain_ref)
    kv_all[0, own_rows, rank : rank + LANES] = jnp.where(
        lane == NOPE + ROPE, 1.0, turned
    ).astype(bf16)
    q_all[own_rows, :] = scaled(q_ref, q_gain_ref)
    pl.semaphore_wait(barrier, count + 2)

    sent = []

    def go(copy):
        copy.start()
        sent.append(copy)
        return copy

    def half_of(h):
        return pl.ds(h * half_rows, half_rows)

    part_rows = (own_rows, cross_rows)

    def kv_forward(step, p):
        return remote(
            kv_all.at[step - 1, part_rows[p]],
            kv_all.at[step, part_rows[p]],
            kvf_send.at[step, p],
            kvf_recv.at[step, p],
            nxt,
        )

    def kv_backward(step, p):
        return remote(
            kv_all.at[(count - step + 1) % count, part_rows[p]],
            kv_all.at[count - step, part_rows[p]],
            kvb_send.at[step, p],
            kvb_recv.at[step, p],
            prv,
        )

    def kv_core(slot, p):
        return remote(
            kv_all.at[slot, part_rows[p]],
            kv_all.at[slot, part_rows[p]],
            kvc_send.at[slot, p],
            kvc_recv.at[slot, p],
            core_peer,
        )

    def forward(step, h):
        src = x_ref.at[half_of(h)] if step == 1 else raw.at[step - 1, half_of(h)]
        return remote(
            src, raw.at[step, half_of(h)], fwd_send.at[step, h], fwd_recv.at[step, h], nxt
        )

    def backward(step, h):
        src = x_ref.at[half_of(h)] if step == 1 else raw.at[count - step + 1, half_of(h)]
        return remote(
            src, raw.at[count - step, half_of(h)], bwd_send.at[step, h], bwd_recv.at[step, h], prv
        )

    def piece(i, slot):
        if i < 4:
            return wgu.at[slot, i // 2, :, pl.ds((i % 2) * fh, fh)]
        return wd.at[i - 4, pl.ds(slot * ff, ff)]

    def own_piece(i):
        if i < 4:
            ref = (gate_ref, up_ref)[i % 2]
            return ref.at[0, :, pl.ds((i // 2) * fh, fh)]
        return down_ref.at[0, :, pl.ds((i - 4) * width, width)]

    kvr, ring = {}, {}
    kvr["x"] = go(
        remote(
            kv_all.at[0, own_rows],
            kv_all.at[0, own_rows],
            kvx_sem.at[0],
            kvx_sem.at[1],
            cross_peer,
        )
    )
    kvr["f", 1, 0] = go(kv_forward(1, 0))
    kvr["b", 1, 0] = go(kv_backward(1, 0))
    kvr["c", 0, 0] = go(kv_core(0, 0))
    q_copies = [
        go(remote(q_all.at[own_rows], q_all.at[own_rows], q_send.at[i], q_recv.at[i], peer))
        for i, peer in enumerate((core_peer, cross_peer, diag_peer))
    ]
    to_coefs = [
        go(
            remote(
                coef_ref,
                coefs.at[step],
                coef_send.at[step],
                coef_recv.at[step],
                (ring_index((place + step) % count, count), tp),
            )
        )
        for step in range(1, count)
    ]
    local, to_core, to_cross, relay = [], [], [], []
    for i in range(4 + chunks):
        to_cross.append(
            go(remote(own_piece(i), piece(i, 2), cross_send.at[i], cross_recv.at[i], cross_peer))
        )
        to_core.append(
            go(remote(own_piece(i), piece(i, 1), core_send.at[i], core_recv.at[i], core_peer))
        )
        copy = pltpu.make_async_copy(own_piece(i), piece(i, 0), local_sem.at[i])
        copy.start()
        local.append(copy)

    def pass_on(i):
        to_cross[i].wait_recv()
        relay.append(
            go(remote(piece(i, 2), piece(i, 3), relay_send.at[i], relay_recv.at[i], core_peer))
        )

    order = [0, half]
    for step in range(1, half):
        order += [step, count - step]

    def base(slot):
        return order.index(slot) * rows

    def norm(slot):
        xn[base(slot) : base(slot) + rows, :] = scaled(
            x_ref if slot == 0 else raw.at[slot], gain_ref
        )

    def coefficient(slot):
        source = coef_ref if slot == 0 else coefs.at[slot]
        line = jnp.broadcast_to(source[pl.ds(me, 1), :], (rows, rows))
        row_id = lax.broadcasted_iota(jnp.int32, (rows, rows), 0)
        col_id = lax.broadcasted_iota(jnp.int32, (rows, rows), 1)
        coef_col[base(slot) : base(slot) + rows, :] = jnp.sum(
            jnp.where(row_id == col_id, line, 0.0), axis=-1, keepdims=True
        )

    w_kv[...] = jnp.zeros_like(w_kv)
    for head in range(heads):
        at = head * LANES
        w_kv[0:rank, at : at + NOPE] = w_key_ref[:, head * NOPE : (head + 1) * NOPE]
        at += head_lanes
        w_kv[0:rank, at : at + VD] = w_value_ref[:, head * VD : (head + 1) * VD]
    pass_row = lax.broadcasted_iota(jnp.int32, (LANES, 2 * head_lanes), 0)
    pass_col = lax.broadcasted_iota(jnp.int32, (LANES, 2 * head_lanes), 1)
    as_key = (
        (pass_col < head_lanes)
        & (pass_col % LANES == pass_row)
        & (pass_row >= NOPE)
        & (pass_row < NOPE + ROPE)
    )
    as_one = (pass_col >= head_lanes) & (pass_col % LANES == VD) & (pass_row == NOPE + ROPE)
    w_kv[rank : rank + LANES, :] = jnp.where(as_key | as_one, 1.0, 0.0).astype(bf16)

    kvr["x"].wait_recv()
    kvr["f", 1, 1] = go(kv_forward(1, 1))
    kvr["b", 1, 1] = go(kv_backward(1, 1))
    kvr["c", 0, 1] = go(kv_core(0, 1))
    ring["f", 1, 0] = go(forward(1, 0))
    ring["b", 1, 0] = go(backward(1, 0))

    wq_cat[...] = jnp.zeros_like(wq_cat)
    for head in range(heads):
        at = head * LANES
        turn = head * ROPE
        wq_cat[:, at : at + NOPE] = w_query_ref[:, head * NOPE : (head + 1) * NOPE]
        wq_cat[:, at + NOPE : at + NOPE + ROPE] = w_rot_ref[:, turn : turn + ROPE]
        at += head_lanes + NOPE
        wq_cat[:, at : at + ROPE // 2] = w_rot_ref[:, turn + ROPE // 2 : turn + ROPE]
        wq_cat[:, at + ROPE // 2 : at + ROPE] = w_rot_ref[:, turn : turn + ROPE // 2]

    for copy in q_copies:
        copy.wait_recv()
    both = jnp.dot(q_all[...], wq_cat[...], preferred_element_type=f32)
    for head in range(heads):
        at = head * LANES
        queries[:, at : at + LANES] = (
            both[:, at : at + LANES] * cos_ref[...]
            + both[:, head_lanes + at : head_lanes + at + LANES] * sin_ref[...]
        ).astype(bf16)
    row_max[...] = jnp.full(row_max.shape, masked_score, f32)
    row_acc[...] = jnp.zeros(row_acc.shape, f32)

    log_scale = (NOPE + ROPE) ** (-0.5) * math.log2(math.e)
    chunk = group_rows // 2

    def work(slot, masked):
        kv_now[...] = jnp.dot(
            kv_all[slot], w_kv[...], preferred_element_type=f32
        ).astype(bf16)

        @pl.loop(0, heads // 2)
        def _(pair):
            for sub in range(2):
                head = pair * 2 + sub
                lanes = pl.ds(pl.multiple_of(head * LANES, LANES), LANES)
                value_lanes = pl.ds(pl.multiple_of(head_lanes + head * LANES, LANES), LANES)
                for first in range(0, group_rows, chunk):
                    part = slice(first, first + chunk)
                    scores = lax.dot_general(
                        queries[part, lanes],
                        kv_now[:, lanes],
                        (((1,), (1,)), ((), ())),
                        preferred_element_type=f32,
                    )
                    if masked:
                        row_id = lax.broadcasted_iota(jnp.int32, scores.shape, 0) + first
                        col_id = lax.broadcasted_iota(jnp.int32, scores.shape, 1)
                        scores = jnp.where(
                            col_id // SEG <= row_id // SEG, scores, masked_score
                        )
                    old = row_max[head, part, :]
                    new = jnp.maximum(old, jnp.max(scores, axis=-1, keepdims=True))
                    weights = jnp.exp2((scores - new[:, :1]) * log_scale).astype(bf16)
                    factor = jnp.exp2((old - new) * log_scale)
                    row_max[head, part, :] = new
                    row_acc[head, part, :] = row_acc[head, part, :] * factor + jnp.dot(
                        weights, kv_now[:, value_lanes], preferred_element_type=f32
                    )

    def attend_slot(slot):
        kvr["c", slot, 0].wait_recv()
        kvr["c", slot, 1].wait_recv()
        if slot == 0:
            work(0, True)
        else:

            @pl.when(ring_index((place + count - slot) % count, count) < me)
            def _():
                work(slot, False)

    def kv_step(step):
        for p in range(2):
            if ("f", step, p) in kvr:
                kvr["f", step, p].wait_recv()
                if step + 1 < half or (step + 1 == half and p == 0):
                    kvr["f", step + 1, p] = go(kv_forward(step + 1, p))
                kvr["c", step, p] = go(kv_core(step, p))
            if ("b", step, p) in kvr:
                kvr["b", step, p].wait_recv()
                if step + 1 < half or (step + 1 == half and p == 1):
                    kvr["b", step + 1, p] = go(kv_backward(step + 1, p))
                kvr["c", count - step, p] = go(kv_core(count - step, p))

    def token_step(step, h):
        ring["f", step, h].wait_recv()
        if step + 1 < half or h == 0:
            ring["f", step + 1, h] = go(forward(step + 1, h))
        ring["b", step, h].wait_recv()
        if step + 1 < half or h == 1:
            ring["b", step + 1, h] = go(backward(step + 1, h))

    tile_rows = 2 * rows

    def hidden(slot_from, slot_to, h, tile_from, tile_to):
        @pl.loop(slot_from, slot_to)
        def _(slot):
            @pl.loop(tile_from, tile_to)
            def _(tile):
                part = pl.ds(pl.multiple_of(tile * tile_rows, tile_rows), tile_rows)
                both = jnp.dot(xn[part, :], wgu[slot, h], preferred_element_type=f32)
                gate = both[:, :fh]
                at = pl.ds(pl.multiple_of((slot * 2 + h) * fh, fh), fh)
                hid[part, at] = (gate * jax.nn.sigmoid(gate) * both[:, fh:]).astype(bf16)

    norm(0)
    coefficient(0)
    attend_slot(0)
    kv_step(1)
    ring["f", 1, 1] = go(forward(1, 1))
    ring["b", 1, 1] = go(backward(1, 1))
    for copy in to_coefs:
        copy.wait_recv()
    for slot in range(1, count):
        coefficient(slot)
    attend_slot(1)
    attend_slot(count - 1)
    for i in range(4):
        local[i].wait()
        to_core[i].wait_recv()
    for step in range(2, half + 1):
        kv_step(step)
        token_step(step - 1, 0)
        attend_slot(step)
        token_step(step - 1, 1)
        if step < half:
            attend_slot(count - step)
        norm(step - 1)
        norm(count - step + 1)
        pass_on(step - 2)
        for h in range(2):
            hidden(0, 2, h, step - 1, step)

    for head in range(heads):
        acc = row_acc[head]
        attended[:, head * VD : (head + 1) * VD] = (
            acc[:, :VD] / acc[:, VD : VD + 1]
        ).astype(bf16)

    @pl.loop(0, 4)
    def _(block):
        part = pl.ds(pl.multiple_of(block * rows, rows), rows)
        mixed[block] = jnp.dot(
            attended[part, :], w_mix_ref[...], preferred_element_type=f32
        ).astype(bf16)

    core_tp = tp + 1 - 2 * (tp % 2)
    mixes = [
        go(
            remote(
                mixed.at[core_tp], from_core.at[0], mix_send.at[0], mix_recv.at[0], core_peer
            )
        ),
        go(
            remote(
                mixed.at[3 - tp], from_core.at[1], mix_send.at[1], mix_recv.at[1], core_peer
            )
        ),
    ]

    def add(target, source):
        target[...] = (target[...].astype(f32) + source[...].astype(f32)).astype(bf16)

    def mix_cross():
        mixes[1].wait_recv()
        add(mixed.at[(tp + 2) % 4], from_core.at[1])
        mixes.append(
            go(
                remote(
                    mixed.at[(tp + 2) % 4], from_cross, mix_send.at[2], mix_recv.at[2], cross_peer
                )
            )
        )

    def mix_end():
        mixes[0].wait_recv()
        mixes[2].wait_recv()
        mix_out_ref[...] = (
            mixed[tp].astype(f32) + from_core[0].astype(f32) + from_cross[...].astype(f32)
        ).astype(bf16)

    pair_count = half
    for i in range(2):
        relay[i].wait_recv()
    hidden(2, 4, 0, 1, pair_count)
    ring["f", half, 0].wait_recv()
    ring["b", half, 1].wait_recv()
    norm(half)
    for h in range(2):
        hidden(0, 2, h, 0, 1)
    hidden(2, 4, 0, 0, 1)
    mix_cross()
    while len(relay) < 4:
        pass_on(len(relay))
    for i in range(2, 4):
        relay[i].wait_recv()
    hidden(2, 4, 1, 0, pair_count)

    def down(c):
        pass_on(4 + c)
        local[4 + c].wait()
        to_core[4 + c].wait_recv()
        relay[4 + c].wait_recv()

        @pl.loop(0, pair_count)
        def _(tile):
            part = pl.ds(pl.multiple_of(tile * tile_rows, tile_rows), tile_rows)
            acc = jnp.dot(hid[part, :], wd[c], preferred_element_type=f32)
            y[c, part, :] = (acc * coef_col[part, :]).astype(bf16)

    def block(slot, h=None):
        if h is None:
            return pl.ds(base(slot), rows)
        return pl.ds(base(slot) + h * half_rows, half_rows)

    sums = {}

    def send_sum(c, k, slot_r, slot_l, h_r=None, h_l=None):
        def landing(ref, h):
            return ref.at[c, k] if h is None else ref.at[c, k, half_of(h)]

        sums["r", c, k] = (
            y.at[c, block(slot_r, h_r)],
            landing(from_prev, h_r),
            sum_r_send.at[c, k],
            sum_r_recv.at[c, k],
            nxt,
        )
        sums["l", c, k] = (
            y.at[c, block(slot_l, h_l)],
            landing(from_next, h_l),
            sum_l_send.at[c, k],
            sum_l_recv.at[c, k],
            prv,
        )

    def start_sum(key):
        sums[key] = go(remote(*sums[key]))

    def sum_start(c):
        send_sum(c, 0, half, half, 0, 1)
        start_sum(("r", c, 0))
        start_sum(("l", c, 0))

    def sum_step(c, k):
        send_sum(c, k, half + k, half - k)
        sums["r", c, k - 1].wait_recv()
        if k == 1:
            add(y.at[c, block(half + k, 0)], from_prev.at[c, 0, half_of(0)])
        else:
            add(y.at[c, block(half + k)], from_prev.at[c, k - 1])
        start_sum(("r", c, k))
        sums["l", c, k - 1].wait_recv()
        if k == 1:
            add(y.at[c, block(half - k, 1)], from_next.at[c, 0, half_of(1)])
        else:
            add(y.at[c, block(half - k)], from_next.at[c, k - 1])
        start_sum(("l", c, k))

    def sum_end(c):
        sums["r", c, half - 1].wait_recv()
        sums["l", c, half - 1].wait_recv()
        out_ref[:, c * width : (c + 1) * width] = (
            y[c, block(0), :].astype(f32)
            + from_prev[c, half - 1].astype(f32)
            + from_next[c, half - 1].astype(f32)
        ).astype(bf16)

    for tick in range(chunks + half):
        for c in range(chunks):
            k = tick - c
            if 1 <= k < half:
                sum_step(c, k)
            elif k == half:
                sum_end(c)
        if tick < chunks:
            down(tick)
            sum_start(tick)
        if tick == chunks + 1:
            mix_end()
    for copy in sent:
        copy.wait_send()


def turn_tables(group_rows):
    half_width = ROPE // 2
    frequency = rope_base ** (-jnp.arange(half_width, dtype=jnp.float32) / half_width)
    positions = lax.axis_index("ep") * group_rows + jnp.arange(group_rows, dtype=jnp.int32)
    angles = positions.astype(jnp.float32)[:, None] * jnp.tile(frequency, LANES // half_width)[None, :]
    lane = jnp.arange(LANES, dtype=jnp.int32)[None, :]
    inside = (lane >= NOPE) & (lane < NOPE + ROPE)
    cosine = jnp.where(inside, jnp.cos(angles), jnp.where(lane < NOPE, 1.0, 0.0))
    sine = jnp.where(inside, jnp.sin(angles), 0.0)
    return cosine, jnp.where(lane < NOPE + half_width, -sine, sine)


def coefficients(expert_ids, route_weights, expert_count):
    experts = jnp.arange(expert_count, dtype=jnp.int32)
    named = expert_ids.T[:, None, :] == experts[None, :, None]
    return jnp.sum(jnp.where(named, route_weights.T[:, None, :], 0.0), axis=0)


def on_device_fused(
    q_latent,
    kv_latent,
    rope_key,
    q_gain,
    kv_gain,
    w_query,
    w_query_rot,
    w_key,
    w_value,
    w_mix_out,
    expert_input,
    ffn_gain,
    expert_ids,
    route_weights,
    w_gate_exp,
    w_up_exp,
    w_down_exp,
):
    count = lax.axis_size("ep")
    chunks = 4
    rows, depth = expert_input.shape
    ff = w_gate_exp.shape[2]
    heads = w_key.shape[1] // NOPE
    rank = kv_latent.shape[1]
    q_rank = q_latent.shape[1]
    group_rows = 4 * rows
    half = count // 2
    width = depth // chunks
    pieces = 4 + chunks
    head_lanes = heads * LANES
    kv_width = rank + LANES
    coef = coefficients(expert_ids, route_weights, count)
    cosine, sine = turn_tables(group_rows)
    bf16, f32 = jnp.bfloat16, jnp.float32
    dma = pltpu.SemaphoreType.DMA
    vmem = pl.BlockSpec(memory_space=pltpu.VMEM)
    hbm = pl.BlockSpec(memory_space=pl.ANY)
    return pl.pallas_call(
        functools.partial(layer_kernel, count, chunks),
        out_shape=[jax.ShapeDtypeStruct((rows, depth), bf16)] * 2,
        in_specs=[vmem] * 15 + [hbm] * 3,
        out_specs=[vmem, vmem],
        scratch_shapes=[
            pltpu.VMEM((group_rows, q_rank), bf16),
            pltpu.VMEM((q_rank, 2 * head_lanes), bf16),
            pltpu.VMEM((group_rows, head_lanes), bf16),
            pltpu.VMEM((count, group_rows, kv_width), bf16),
            pltpu.VMEM((kv_width, 2 * head_lanes), bf16),
            pltpu.VMEM((group_rows, 2 * head_lanes), bf16),
            pltpu.VMEM((heads, group_rows, LANES), f32),
            pltpu.VMEM((heads, group_rows, LANES), f32),
            pltpu.VMEM((group_rows, heads * VD), bf16),
            pltpu.VMEM((4, rows, depth), bf16),
            pltpu.VMEM((2, rows, depth), bf16),
            pltpu.VMEM((rows, depth), bf16),
            pltpu.VMEM((count, rows, depth), bf16),
            pltpu.VMEM((count * rows, depth), bf16),
            pltpu.VMEM((4, 2, depth, ff), bf16),
            pltpu.VMEM((chunks, 4 * ff, width), bf16),
            pltpu.VMEM((count * rows, 4 * ff), bf16),
            pltpu.VMEM((chunks, count * rows, width), bf16),
            pltpu.VMEM((chunks, half, rows, width), bf16),
            pltpu.VMEM((chunks, half, rows, width), bf16),
            pltpu.VMEM((count, count, rows), f32),
            pltpu.VMEM((count * rows, 1), f32),
            dma((3,)),
            dma((3,)),
            dma((2,)),
            dma((half + 1, 2)),
            dma((half + 1, 2)),
            dma((half + 1, 2)),
            dma((half + 1, 2)),
            dma((count, 2)),
            dma((count, 2)),
            dma((3,)),
            dma((3,)),
            dma((pieces,)),
            dma((count,)),
            dma((count,)),
            dma((half + 1, 2)),
            dma((half + 1, 2)),
            dma((half + 1, 2)),
            dma((half + 1, 2)),
            dma((pieces,)),
            dma((pieces,)),
            dma((pieces,)),
            dma((pieces,)),
            dma((pieces,)),
            dma((pieces,)),
            dma((chunks, half)),
            dma((chunks, half)),
            dma((chunks, half)),
            dma((chunks, half)),
        ],
        compiler_params=pltpu.CompilerParams(
            collective_id=0, has_side_effects=True, vmem_limit_bytes=63 * 1024 * 1024
        ),
        cost_estimate=pl.CostEstimate(
            flops=6 * count * rows * depth * 4 * ff,
            bytes_accessed=12 * depth * ff * 2,
            transcendentals=count * rows * 4 * ff,
        ),
        name="layer",
    )(
        q_latent,
        kv_latent,
        rope_key,
        q_gain.reshape(1, -1),
        kv_gain.reshape(1, -1),
        w_query,
        w_query_rot,
        w_key,
        w_value,
        w_mix_out,
        cosine,
        sine,
        expert_input,
        ffn_gain.reshape(1, -1),
        coef,
        w_gate_exp,
        w_up_exp,
        w_down_exp,
    )


def fits(mesh):
    ep, tp = mesh.shape["ep"], mesh.shape["tp"]
    return tp == 4 and ep % 2 == 0 and 4 <= ep <= 8


def solution(mesh):
    return jax.shard_map(
        on_device_fused if fits(mesh) else on_device_plain,
        mesh=mesh,
        in_specs=(
            P(("ep", "tp"), None),
            P(("ep", "tp"), None),
            P(("ep", "tp"), None),
            P(),
            P(),
            P(None, "tp"),
            P(None, "tp"),
            P(None, "tp"),
            P(None, "tp"),
            P("tp", None),
            P(("ep", "tp"), None),
            P(),
            P(("ep", "tp"), None),
            P(("ep", "tp"), None),
            P("ep", None, "tp"),
            P("ep", None, "tp"),
            P("ep", "tp", None),
        ),
        out_specs=(P(("ep", "tp"), None), P(("ep", "tp"), None)),
        check_vma=False,
    )
```

```python
import functools
import math

import jax
import jax.numpy as jnp
import numpy as np
from jax import lax
from jax.experimental import pallas as pl
from jax.experimental.pallas import tpu as pltpu
from jax.sharding import PartitionSpec as P

D = 2048
NOPE = 64
ROPE = 32
VD = 64
TOPK = 4
SEG = 64


norm_epsilon = 1e-06
rope_base = 10000.0
masked_score = -1e30


def rms_scale(values_in, gain_vec):
    floats = values_in.astype(jnp.float32)
    return (
        floats
        * lax.rsqrt(jnp.mean(floats * floats, axis=-1, keepdims=True) + norm_epsilon)
        * gain_vec
    )


def tables(positions):
    half_width = ROPE // 2
    frequency = rope_base ** (-jnp.arange(half_width, dtype=jnp.float32) / half_width)
    angles = positions.astype(jnp.float32)[:, None] * frequency[None, :]
    return (jnp.cos(angles), jnp.sin(angles))


def rotate_pairs(values_in, cosine, sine_table):
    half_width = values_in.shape[-1] // 2
    first, second = (values_in[..., :half_width], values_in[..., half_width:])
    return jnp.concatenate(
        [first * cosine - second * sine_table, first * sine_table + second * cosine], axis=-1
    )


LANES = 128


def pad_heads(weight, heads, width):
    split = weight.reshape(weight.shape[0], heads, width)
    return jnp.pad(split, ((0, 0), (0, 0), (0, LANES - width))).reshape(
        weight.shape[0], heads * LANES
    )


def make_queries(q_rows, q_gain, w_query, w_query_rot, heads, group_rows):
    start = lax.axis_index("ep") * group_rows
    cosine, sine_table = tables(start + jnp.arange(group_rows, dtype=jnp.int32))
    normed = rms_scale(q_rows, q_gain).astype(jnp.bfloat16)
    plain = jnp.dot(normed, w_query, preferred_element_type=jnp.float32).astype(jnp.bfloat16)
    turned = jnp.dot(normed, w_query_rot, preferred_element_type=jnp.float32).reshape(
        group_rows, heads, ROPE
    )
    turned = rotate_pairs(turned, cosine[:, None, :], sine_table[:, None, :]).astype(jnp.bfloat16)
    blank = jnp.zeros((group_rows, heads, LANES - NOPE - ROPE), jnp.bfloat16)
    joined = jnp.concatenate([plain.reshape(group_rows, heads, NOPE), turned, blank], axis=-1)
    return joined.reshape(group_rows, heads * LANES)


def make_keys(kv_rows, kv_gain, w_key, w_value, heads):
    row_count = kv_rows.shape[0]
    rank = w_key.shape[0]
    normed = rms_scale(kv_rows[:, :rank], kv_gain).astype(jnp.bfloat16)
    cosine, sine_table = tables(jnp.arange(row_count, dtype=jnp.int32))
    turned = rotate_pairs(kv_rows[:, rank:].astype(jnp.float32), cosine, sine_table)
    turned = jnp.pad(
        turned.astype(jnp.bfloat16), ((0, 0), (NOPE, LANES - NOPE - ROPE))
    )
    plain = jnp.dot(normed, pad_heads(w_key, heads, NOPE), preferred_element_type=jnp.float32)
    keys = plain.astype(jnp.bfloat16) + jnp.tile(turned, (1, heads))
    raw = jnp.dot(normed, pad_heads(w_value, heads, VD), preferred_element_type=jnp.float32)
    ones = (jnp.arange(heads * LANES, dtype=jnp.int32) % LANES == VD).astype(jnp.bfloat16)
    return keys, raw.astype(jnp.bfloat16) + ones[None, :]


def attention_kernel(heads, chunk, group_ref, q_ref, k_ref, v_ref, o_ref, max_ref, acc_ref):
    step = pl.program_id(0)
    group = group_ref[0]
    rows = q_ref.shape[0]
    keys = k_ref.shape[0]
    log_scale = (NOPE + ROPE) ** (-0.5) * math.log2(math.e)

    @pl.when(step == 0)
    def _():
        max_ref[...] = jnp.full(max_ref.shape, masked_score, jnp.float32)
        acc_ref[...] = jnp.zeros(acc_ref.shape, jnp.float32)

    def work(masked):
        for head in range(heads):
            lanes = slice(head * LANES, (head + 1) * LANES)
            for first in range(0, rows, chunk):
                part = slice(first, first + chunk)
                scores = lax.dot_general(
                    q_ref[part, lanes],
                    k_ref[:, lanes],
                    (((1,), (1,)), ((), ())),
                    preferred_element_type=jnp.float32,
                )
                if masked:
                    row_id = lax.broadcasted_iota(jnp.int32, (chunk, keys), 0) + first
                    col_id = lax.broadcasted_iota(jnp.int32, (chunk, keys), 1)
                    scores = jnp.where(col_id // SEG <= row_id // SEG, scores, masked_score)
                old = max_ref[head, part, :]
                new = jnp.maximum(old, jnp.max(scores, axis=-1, keepdims=True))
                weights = jnp.exp2((scores - new[:, :1]) * log_scale).astype(jnp.bfloat16)
                factor = jnp.exp2((old - new) * log_scale)
                max_ref[head, part, :] = new
                acc_ref[head, part, :] = acc_ref[head, part, :] * factor + jnp.dot(
                    weights, v_ref[:, lanes], preferred_element_type=jnp.float32
                )

    @pl.when(step < group)
    def _():
        work(False)

    @pl.when(step == group)
    def _():
        work(True)

    @pl.when(step == pl.num_programs(0) - 1)
    def _():
        for head in range(heads):
            acc = acc_ref[head]
            o_ref[:, head * VD : (head + 1) * VD] = (
                acc[:, :VD] / acc[:, VD : VD + 1]
            ).astype(jnp.bfloat16)


def attend(queries, keys, values, heads, group_rows):
    group = lax.axis_index("ep").astype(jnp.int32).reshape(1)
    blocks = keys.shape[0] // group_rows
    width = heads * LANES
    chunk = 256 if group_rows % 256 == 0 else group_rows
    return pl.pallas_call(
        functools.partial(attention_kernel, heads, chunk),
        out_shape=jax.ShapeDtypeStruct((group_rows, heads * VD), jnp.bfloat16),
        grid_spec=pltpu.PrefetchScalarGridSpec(
            num_scalar_prefetch=1,
            grid=(blocks,),
            in_specs=[
                pl.BlockSpec((group_rows, width), lambda i, g: (0, 0)),
                pl.BlockSpec((group_rows, width), lambda i, g: (jnp.minimum(i, g[0]), 0)),
                pl.BlockSpec((group_rows, width), lambda i, g: (jnp.minimum(i, g[0]), 0)),
            ],
            out_specs=pl.BlockSpec((group_rows, heads * VD), lambda i, g: (0, 0)),
            scratch_shapes=[
                pltpu.VMEM((heads, group_rows, LANES), jnp.float32),
                pltpu.VMEM((heads, group_rows, LANES), jnp.float32),
            ],
        ),
        compiler_params=pltpu.CompilerParams(
            dimension_semantics=("arbitrary",), vmem_limit_bytes=24 * 1024 * 1024
        ),
        cost_estimate=pl.CostEstimate(
            flops=4 * heads * group_rows * keys.shape[0] * LANES * 2,
            bytes_accessed=4 * keys.shape[0] * width,
            transcendentals=heads * group_rows * keys.shape[0],
        ),
        name="attend",
    )(group, queries, keys, values)


def on_device_plain(
    q_latent,
    kv_latent,
    rope_key,
    q_gain,
    kv_gain,
    w_query,
    w_query_rot,
    w_key,
    w_value,
    w_mix_out,
    expert_input,
    ffn_gain,
    expert_ids,
    route_weights,
    w_gate_exp,
    w_up_exp,
    w_down_exp,
):
    tok_rows = q_latent.shape[0]
    tp_count = lax.axis_size("tp")
    expert_count = lax.axis_size("ep")
    slot_count = 3 * tok_rows * TOPK // (2 * expert_count)
    group_rows = tp_count * tok_rows
    heads_here = w_key.shape[1] // NOPE

    gate_all = lax.all_gather(w_gate_exp[0], "tp", axis=0)
    up_all = lax.all_gather(w_up_exp[0], "tp", axis=0)
    down_all = lax.all_gather(w_down_exp[0], "tp", axis=0)

    normed = rms_scale(expert_input, ffn_gain).astype(jnp.bfloat16)
    routed = expert_ids.reshape(-1)
    onehot = (routed[:, None] == jnp.arange(expert_count, dtype=jnp.int32)[None, :]).astype(
        jnp.int32
    )
    slot_number = jnp.sum((jnp.cumsum(onehot, axis=0) - 1) * onehot, axis=-1)
    slot_place = (routed * slot_count + slot_number).reshape(tok_rows, TOPK)
    slot_line = jnp.arange(expert_count * slot_count, dtype=jnp.int32)
    picks = [
        (slot_place[:, route_rank][:, None] == slot_line[None, :]).astype(jnp.bfloat16)
        for route_rank in range(TOPK)
    ]
    dispatch = picks[0]
    for route_rank in range(1, TOPK):
        dispatch = dispatch + picks[route_rank]
    outgoing = lax.dot_general(
        dispatch, normed, (((0,), (0,)), ((), ())), preferred_element_type=jnp.float32
    ).astype(jnp.bfloat16)
    arrived = lax.all_to_all(
        outgoing.reshape(expert_count, slot_count, D), "ep", split_axis=0, concat_axis=0, tiled=True
    )
    rows = arrived.reshape(expert_count * slot_count, D)

    own_rows = jnp.concatenate([kv_latent, rope_key], axis=1)
    ep_rows = lax.all_gather(own_rows, "ep", axis=0, tiled=True)
    column_count = own_rows.shape[1]
    piece_width = column_count // 3 if column_count % 3 == 0 else column_count
    pieces = [
        lax.all_gather(ep_rows[:, first : first + piece_width], "tp", axis=0)
        for first in range(0, column_count, piece_width)
    ]
    kv_rows = (
        jnp.concatenate(pieces, axis=2)
        .reshape(tp_count, expert_count, tok_rows, column_count)
        .transpose(1, 0, 2, 3)
        .reshape(expert_count * group_rows, column_count)
    )
    q_rows = lax.all_gather(q_latent, "tp", axis=0, tiled=True)
    queries = make_queries(q_rows, q_gain, w_query, w_query_rot, heads_here, group_rows)
    keys, values = make_keys(kv_rows, kv_gain, w_key, w_value, heads_here)
    attention = attend(queries, keys, values, heads_here, group_rows)

    total = jnp.zeros((rows.shape[0], D), jnp.float32)
    for block in range(tp_count):
        gate_part = jnp.dot(rows, gate_all[block], preferred_element_type=jnp.float32)
        up_part = jnp.dot(rows, up_all[block], preferred_element_type=jnp.float32)
        hidden = (jax.nn.silu(gate_part) * up_part).astype(jnp.bfloat16)
        part = jnp.dot(hidden, down_all[block], preferred_element_type=jnp.float32)
        total = total + part.astype(jnp.bfloat16).astype(jnp.float32)
    summed = total.astype(jnp.bfloat16)
    results = lax.all_to_all(
        summed.reshape(expert_count, slot_count, D), "ep", split_axis=0, concat_axis=0, tiled=True
    ).reshape(expert_count * slot_count, D)

    partial_out = jnp.dot(attention, w_mix_out, preferred_element_type=jnp.float32).astype(
        jnp.bfloat16
    )
    mixer_out = lax.psum_scatter(partial_out, "tp", scatter_dimension=0, tiled=True)

    fetched = jnp.dot(
        jnp.concatenate(picks, axis=0), results, preferred_element_type=jnp.float32
    ).astype(jnp.bfloat16)
    combined = jnp.zeros((tok_rows, D), jnp.float32)
    for route_rank in range(TOPK):
        piece = fetched[route_rank * tok_rows : (route_rank + 1) * tok_rows].astype(jnp.float32)
        combined = combined + route_weights[:, route_rank : route_rank + 1] * piece
    return (mixer_out, combined.astype(jnp.bfloat16))


MESH = pl.DeviceIdType.MESH
VR = VD + 16


def ring_place(index, count):
    side = index % 2
    line = index // 2
    return line + side * (count - 1 - 2 * line)


def ring_index(place, count):
    side = place // (count // 2)
    line = place + side * (count - 1 - 2 * place)
    return 2 * line + side


def remote(src, dst, send, recv, device):
    return pltpu.make_async_remote_copy(
        src_ref=src, dst_ref=dst, send_sem=send, recv_sem=recv, device_id=device, device_id_type=MESH
    )


def sum_plan(chunks, half):
    block = 11.2 / chunks
    lag = 1.7
    now, link = 0.0, 0.0
    arrive, plan = {}, []
    downs, side = 0, [("cross", 12.0), ("close", 34.0)]
    while downs < chunks or arrive or side:
        ready = sorted((k, c) for (c, k), at in arrive.items() if at <= now)
        can_down = downs < chunks and downs * 22.4 / chunks <= now
        if side and side[0][1] <= now:
            plan.append((side.pop(0)[0], 0, 0))
        elif can_down and (link > now + 0.4 or not ready):
            plan.append(("down", downs, 0))
            link = max(link, now + 0.4) + block / 2
            arrive[downs, 1] = link + lag
            now += 10.0 / chunks
            downs += 1
        elif ready:
            k, c = ready[0]
            del arrive[c, k]
            now += 0.1
            if k < half:
                plan.append(("step", c, k))
                link = max(link, now) + block
                arrive[c, k + 1] = link + lag
            else:
                plan.append(("end", c, k))
        else:
            times = list(arrive.values()) + [at for _, at in side]
            if downs < chunks:
                times.append(downs * 22.4 / chunks)
            now = max(now + 0.01, min(times))
    return plan


def layer_kernel(
    count,
    chunks,
    q_ref,
    kv_ref,
    rope_ref,
    q_gain_ref,
    kv_gain_ref,
    w_query_ref,
    w_rot_ref,
    w_key_ref,
    w_value_ref,
    w_mix_ref,
    freq_ref,
    x_ref,
    gain_ref,
    ids_ref,
    route_ref,
    gate_ref,
    up_ref,
    down_ref,
    mix_out_ref,
    out_ref,
    x_now,
    w_query_now,
    w_rot_now,
    w_key_now,
    w_value_now,
    w_mix_now,
    mix_stage,
    out_stage,
    cos_ref,
    sin_ref,
    coef_ref,
    q_all,
    wq_cat,
    queries,
    kv_all,
    w_kv,
    w_vt,
    k_now,
    v_now,
    row_max,
    row_acc,
    attended,
    mixed,
    from_core,
    from_cross,
    raw,
    xn,
    wgu,
    wd,
    hid,
    y,
    from_prev,
    from_next,
    coefs,
    coef_col,
    q_send,
    q_recv,
    kvx_sem,
    kvf_send,
    kvf_recv,
    kvb_send,
    kvb_recv,
    kvc_send,
    kvc_recv,
    mix_send,
    mix_recv,
    in_sem,
    out_sem,
    local_sem,
    coef_send,
    coef_recv,
    fwd_send,
    fwd_recv,
    bwd_send,
    bwd_recv,
    core_send,
    core_recv,
    cross_send,
    cross_recv,
    relay_send,
    relay_recv,
    sum_r_send,
    sum_r_recv,
    sum_l_send,
    sum_l_recv,
):
    bf16, f32 = jnp.bfloat16, jnp.float32
    rows = x_ref.shape[0]
    half_rows = rows // 2
    half = count // 2
    ff = gate_ref.shape[2]
    fh = ff // 2
    width = out_ref.shape[1] // chunks
    group_rows = 4 * rows
    heads = w_key_ref.shape[1] // NOPE
    rank = kv_ref.shape[1]
    head_lanes = heads * LANES
    me = lax.axis_index("ep")
    tp = lax.axis_index("tp")
    place = ring_place(me, count)
    nxt = (ring_index((place + 1) % count, count), tp)
    prv = (ring_index((place + count - 1) % count, count), tp)
    core_peer = (me, tp + 1 - 2 * (tp % 2))
    cross_peer = (me, (tp + 2) % 4)

    barrier = pltpu.get_barrier_semaphore()
    for step in range(1, count):
        pl.semaphore_signal(
            barrier,
            inc=1,
            device_id=(ring_index((place + step) % count, count), tp),
            device_id_type=MESH,
        )
    for peer in (core_peer, cross_peer):
        pl.semaphore_signal(barrier, inc=1, device_id=peer, device_id_type=MESH)

    inputs = []
    for i, (src, dst) in enumerate(
        (
            (x_ref, x_now),
            (w_key_ref, w_key_now),
            (w_value_ref, w_value_now),
            (w_query_ref, w_query_now),
            (w_rot_ref, w_rot_now),
            (w_mix_ref, w_mix_now),
        )
    ):
        inputs.append(pltpu.make_async_copy(src, dst, in_sem.at[i]))
        inputs[-1].start()

    def rows_of(index):
        return pl.ds(pl.multiple_of(index * rows, rows), rows)

    own_rows, cross_rows = rows_of(tp), rows_of((tp + 2) % 4)

    def scaled(ref, gain):
        floats = ref[...].astype(f32)
        scale = lax.rsqrt(jnp.mean(floats * floats, axis=-1, keepdims=True) + norm_epsilon)
        return (floats * scale * gain[...]).astype(bf16)

    def turn_table(first, size):
        lane = lax.broadcasted_iota(jnp.int32, (size, LANES), 1)
        row = lax.broadcasted_iota(jnp.int32, (size, LANES), 0)
        angle = (me * group_rows + first + row).astype(f32) * freq_ref[...]
        inside = (lane >= NOPE) & (lane < NOPE + ROPE)
        sine = jnp.where(inside, jnp.sin(angle), 0.0)
        return (
            jnp.where(inside, jnp.cos(angle), jnp.where(lane < NOPE, 1.0, 0.0)),
            jnp.where(lane < NOPE + ROPE // 2, -sine, sine),
        )

    turn_row = lax.broadcasted_iota(jnp.int32, (ROPE, LANES), 0)
    turn_col = lax.broadcasted_iota(jnp.int32, (ROPE, LANES), 1) - NOPE
    straight = (turn_row == turn_col).astype(f32).astype(bf16)
    swapped = (
        ((turn_row == turn_col + ROPE // 2) & (turn_col < ROPE // 2))
        | ((turn_row == turn_col - ROPE // 2) & (turn_col >= ROPE // 2))
    )
    swapped = jnp.where(swapped, 1.0, 0.0).astype(bf16)
    rope = rope_ref[...]
    own_cos, own_sin = turn_table(tp * rows, rows)
    by_column = (((0,), (0,)), ((), ()))
    turned = (
        lax.dot_general(rope, straight, by_column, preferred_element_type=f32) * own_cos
        + lax.dot_general(rope, swapped, by_column, preferred_element_type=f32) * own_sin
    )
    lane = lax.broadcasted_iota(jnp.int32, (rows, LANES), 1)
    kv_all[0, own_rows, 0:rank] = scaled(kv_ref, kv_gain_ref)
    kv_all[0, own_rows, rank : rank + LANES] = jnp.where(
        lane == NOPE + ROPE, 1.0, turned
    ).astype(bf16)
    q_all[own_rows, :] = scaled(q_ref, q_gain_ref)
    expert_id = lax.broadcasted_iota(jnp.int32, (count, rows), 0)
    coef = jnp.zeros((count, rows), f32)
    for k in range(TOPK):
        coef += jnp.where(ids_ref[k : k + 1, :] == expert_id, route_ref[k : k + 1, :], 0.0)
    coef_ref[...] = coef
    pl.semaphore_wait(barrier, count + 1)

    def go(copy):
        copy.start()
        return copy

    def half_of(h):
        return pl.ds(h * half_rows, half_rows)

    part_rows = (own_rows, cross_rows)

    def kv_forward(step, p):
        return remote(
            kv_all.at[step - 1, part_rows[p]],
            kv_all.at[step, part_rows[p]],
            kvf_send,
            kvf_recv.at[step - 1, p],
            nxt,
        )

    def kv_backward(step, p):
        return remote(
            kv_all.at[(count - step + 1) % count, part_rows[p]],
            kv_all.at[count - step, part_rows[p]],
            kvb_send,
            kvb_recv.at[step - 1, p],
            prv,
        )

    def kv_core(slot, p):
        return remote(
            kv_all.at[slot, part_rows[p]],
            kv_all.at[slot, part_rows[p]],
            kvc_send,
            kvc_recv.at[slot, p],
            core_peer,
        )

    def forward(step, h):
        src = x_ref.at[half_of(h)] if step == 1 else raw.at[step - 1, half_of(h)]
        return remote(
            src, raw.at[step, half_of(h)], fwd_send, fwd_recv.at[step - 1, h], nxt
        )

    def backward(step, h):
        src = x_ref.at[half_of(h)] if step == 1 else raw.at[count - step + 1, half_of(h)]
        return remote(
            src, raw.at[count - step, half_of(h)], bwd_send, bwd_recv.at[step - 1, h], prv
        )

    def piece(i, slot):
        if i < 4:
            return wgu.at[slot, i // 2, :, pl.ds((i % 2) * fh, fh)]
        return wd.at[i - 4, pl.ds(slot * ff, ff)]

    def own_piece(i):
        if i < 4:
            ref = (gate_ref, up_ref)[i % 2]
            return ref.at[0, :, pl.ds((i // 2) * fh, fh)]
        return down_ref.at[0, :, pl.ds((i - 4) * width, width)]

    kvr, ring = {}, {}
    kvr["x"] = go(
        remote(
            kv_all.at[0, own_rows],
            kv_all.at[0, own_rows],
            kvx_sem.at[0],
            kvx_sem.at[1],
            cross_peer,
        )
    )
    kvr["f", 1, 0] = go(kv_forward(1, 0))
    kvr["b", 1, 0] = go(kv_backward(1, 0))
    kvr["c", 0, 0] = go(kv_core(0, 0))
    q_copies = [
        go(remote(q_all.at[own_rows], q_all.at[own_rows], q_send.at[i], q_recv.at[i], peer))
        for i, peer in enumerate((core_peer, cross_peer))
    ]
    ring["f", 1, 0] = go(forward(1, 0))
    ring["b", 1, 1] = go(backward(1, 1))
    to_coefs = [
        go(
            remote(
                coef_ref,
                coefs.at[step],
                coef_send,
                coef_recv,
                (ring_index((place + step) % count, count), tp),
            )
        )
        for step in range(1, count)
    ]
    local, to_core, to_cross, relay = [], [], [], []
    for i in range(4 + chunks):
        to_cross.append(
            go(remote(own_piece(i), piece(i, 2), cross_send, cross_recv.at[i], cross_peer))
        )
        to_core.append(
            go(remote(own_piece(i), piece(i, 1), core_send, core_recv.at[i], core_peer))
        )
        copy = pltpu.make_async_copy(own_piece(i), piece(i, 0), local_sem.at[i])
        copy.start()
        local.append(copy)

    def pass_on(i):
        to_cross[i].wait_recv()
        relay.append(
            go(remote(piece(i, 2), piece(i, 3), relay_send, relay_recv.at[i], core_peer))
        )

    order = [0, half]
    for step in range(1, half):
        order += [step, count - step]

    def base(slot):
        return order.index(slot) * rows

    def norm(slot):
        xn[base(slot) : base(slot) + rows, :] = scaled(
            x_now if slot == 0 else raw.at[slot], gain_ref
        )

    def coefficient(slot):
        source = coef_ref if slot == 0 else coefs.at[slot]
        line = jnp.broadcast_to(source[pl.ds(me, 1), :], (rows, rows))
        row_id = lax.broadcasted_iota(jnp.int32, (rows, rows), 0)
        col_id = lax.broadcasted_iota(jnp.int32, (rows, rows), 1)
        coef_col[base(slot) : base(slot) + rows, :] = jnp.sum(
            jnp.where(row_id == col_id, line, 0.0), axis=-1, keepdims=True
        )

    w_kv[...] = jnp.zeros_like(w_kv)
    inputs[1].wait()
    for head in range(heads):
        at = head * LANES
        w_kv[0:rank, at : at + NOPE] = w_key_now[:, head * NOPE : (head + 1) * NOPE]
    pass_row = lax.broadcasted_iota(jnp.int32, (LANES, head_lanes), 0)
    pass_col = lax.broadcasted_iota(jnp.int32, (LANES, head_lanes), 1)
    as_key = (
        (pass_col % LANES == pass_row) & (pass_row >= NOPE) & (pass_row < NOPE + ROPE)
    )
    w_kv[rank : rank + LANES, :] = jnp.where(as_key, 1.0, 0.0).astype(bf16)

    kvr["x"].wait_recv()
    kvr["f", 1, 1] = go(kv_forward(1, 1))
    kvr["b", 1, 1] = go(kv_backward(1, 1))
    kvr["c", 0, 1] = go(kv_core(0, 1))

    cos_ref[...], sin_ref[...] = turn_table(0, group_rows)
    wq_cat[...] = jnp.zeros_like(wq_cat)
    inputs[3].wait()
    inputs[4].wait()
    for head in range(heads):
        at = head * LANES
        turn = head * ROPE
        wq_cat[:, at : at + NOPE] = w_query_now[:, head * NOPE : (head + 1) * NOPE]
        wq_cat[:, at + NOPE : at + NOPE + ROPE] = w_rot_now[:, turn : turn + ROPE]
        at += head_lanes + NOPE
        wq_cat[:, at : at + ROPE // 2] = w_rot_now[:, turn + ROPE // 2 : turn + ROPE]
        wq_cat[:, at + ROPE // 2 : at + ROPE] = w_rot_now[:, turn : turn + ROPE // 2]

    inputs[2].wait()
    flipped = jnp.transpose(w_value_now[...].astype(f32)).astype(bf16)
    one_row = lax.broadcasted_iota(jnp.int32, (VR, rank + LANES), 0)
    one_col = lax.broadcasted_iota(jnp.int32, (VR, rank + LANES), 1)
    ones = ((one_row == VD) & (one_col == rank + NOPE + ROPE)).astype(f32).astype(bf16)
    for head in range(heads):
        w_vt[head * VR : (head + 1) * VR, :] = ones
        w_vt[head * VR : head * VR + VD, 0:rank] = flipped[head * VD : (head + 1) * VD, :]
    inputs[0].wait()
    norm(0)
    coefficient(0)
    row_max[...] = jnp.full(row_max.shape, masked_score, f32)
    row_acc[...] = jnp.zeros(row_acc.shape, f32)
    q_copies[1].wait_recv()
    q_copies.append(
        go(
            remote(
                q_all.at[cross_rows], q_all.at[cross_rows], q_send.at[2], q_recv.at[2], core_peer
            )
        )
    )

    def make_queries_here():
        q_copies[0].wait_recv()
        q_copies[2].wait_recv()
        both = jnp.dot(q_all[...], wq_cat[...], preferred_element_type=f32)
        for head in range(heads):
            at = head * LANES
            queries[:, at : at + LANES] = (
                both[:, at : at + LANES] * cos_ref[...]
                + both[:, head_lanes + at : head_lanes + at + LANES] * sin_ref[...]
            ).astype(bf16)

    log_scale = (NOPE + ROPE) ** (-0.5) * math.log2(math.e)

    def work(slot, masked):
        k_now[...] = jnp.dot(kv_all[slot], w_kv[...], preferred_element_type=f32).astype(bf16)
        turned_values = lax.dot_general(
            w_vt[...], kv_all[slot], (((1,), (1,)), ((), ())), preferred_element_type=f32
        )
        v_now[...] = turned_values.astype(bf16).reshape(heads, VR, group_rows)

        @pl.loop(0, heads // 2)
        def _(pair):
            for sub in range(2):
                head = pair * 2 + sub
                lanes = pl.ds(pl.multiple_of(head * LANES, LANES), LANES)
                scores = lax.dot_general(
                    k_now[:, lanes],
                    queries[:, lanes],
                    (((1,), (1,)), ((), ())),
                    preferred_element_type=f32,
                )
                if masked:
                    key_id = lax.broadcasted_iota(jnp.int32, scores.shape, 0)
                    query_id = lax.broadcasted_iota(jnp.int32, scores.shape, 1)
                    scores = jnp.where(key_id // SEG <= query_id // SEG, scores, masked_score)
                old = row_max[head]
                new = jnp.maximum(old, jnp.max(scores, axis=0, keepdims=True))
                weights = jnp.exp2((scores - new) * log_scale).astype(bf16)
                factor = jnp.exp2((old - new) * log_scale)
                row_max[head] = new
                row_acc[head] = row_acc[head] * factor + jnp.dot(
                    v_now[head], weights, preferred_element_type=f32
                )

    def attend_slot(slot):
        kvr["c", slot, 0].wait_recv()
        kvr["c", slot, 1].wait_recv()
        if slot == 0:
            work(0, True)
        else:

            @pl.when(ring_index((place + count - slot) % count, count) < me)
            def _():
                work(slot, False)

    def kv_step(step, p):
        if step < half or p == 0:
            kvr["f", step, p].wait_recv()
            if step + 1 < half or (step + 1 == half and p == 0):
                kvr["f", step + 1, p] = go(kv_forward(step + 1, p))
            kvr["c", step, p] = go(kv_core(step, p))
        if step < half or p == 1:
            kvr["b", step, p].wait_recv()
            if step + 1 < half or (step + 1 == half and p == 1):
                kvr["b", step + 1, p] = go(kv_backward(step + 1, p))
            kvr["c", count - step, p] = go(kv_core(count - step, p))

    def token_wait(step, i):
        ring["f", step, i].wait_recv()
        ring["b", step, 1 - i].wait_recv()

    def token_pass(step, i):
        if step + 1 < half or i == 0:
            ring["f", step + 1, i] = go(forward(step + 1, i))
            ring["b", step + 1, 1 - i] = go(backward(step + 1, 1 - i))

    def token_step(step, i):
        token_wait(step, i)
        token_pass(step, i)

    tile_rows = 2 * rows

    def hidden(slot_from, slot_to, halves, first, size, tiles=1):
        @pl.loop(slot_from, slot_to)
        def _(slot):
            @pl.loop(0, tiles)
            def _(tile):
                part = pl.ds(pl.multiple_of(first + tile * size, rows), size)
                for h in halves:
                    both = jnp.dot(xn[part, :], wgu[slot, h], preferred_element_type=f32)
                    gate = both[:, :fh]
                    at = pl.ds(pl.multiple_of((slot * 2 + h) * fh, fh), fh)
                    hid[part, at] = (gate * jax.nn.sigmoid(gate) * both[:, fh:]).astype(bf16)

    def pair_norm(step):
        norm(step)
        norm(count - step)

    def pair_first(step):
        return base(step)

    mixes = []

    def mix_start():
        for head in range(heads):
            acc = row_acc[head]
            attended[head * VD : (head + 1) * VD, :] = (
                acc[:VD, :] / acc[VD : VD + 1, :]
            ).astype(bf16)
        inputs[5].wait()

        @pl.loop(0, 4)
        def _(block):
            part = pl.ds(pl.multiple_of(block * rows, rows), rows)
            mixed[block] = lax.dot_general(
                attended[:, part], w_mix_now[...], by_column, preferred_element_type=f32
            ).astype(bf16)

        for i, index in enumerate((3 - tp, tp + 1 - 2 * (tp % 2))):
            mixes.append(
                go(
                    remote(
                        mixed.at[index], from_core.at[i], mix_send.at[i], mix_recv.at[i], core_peer
                    )
                )
            )

    def add(target, source):
        target[...] = (target[...].astype(f32) + source[...].astype(f32)).astype(bf16)

    def mix_cross():
        mixes[0].wait_recv()
        add(mixed.at[(tp + 2) % 4], from_core.at[0])
        mixes.append(
            go(
                remote(
                    mixed.at[(tp + 2) % 4], from_cross, mix_send.at[2], mix_recv.at[2], cross_peer
                )
            )
        )

    outs = []

    def mix_end():
        mixes[1].wait_recv()
        mixes[2].wait_recv()
        mix_stage[...] = (
            mixed[tp].astype(f32) + from_core[1].astype(f32) + from_cross[...].astype(f32)
        ).astype(bf16)
        outs.append(pltpu.make_async_copy(mix_stage, mix_out_ref, out_sem.at[chunks]))
        outs[-1].start()

    def down(c):
        local[4 + c].wait()
        to_core[4 + c].wait_recv()
        relay[4 + c].wait_recv()

        def tile(pair):
            part = pl.ds(pl.multiple_of(pair * tile_rows, tile_rows), tile_rows)
            acc = jnp.dot(hid[part, :], wd[c], preferred_element_type=f32)
            y[c, part, :] = (acc * coef_col[part, :]).astype(bf16)

        tile(0)
        sum_start(c)

        @pl.loop(1, half)
        def _(back):
            tile(half - back)

    def block(slot, h=None):
        if h is None:
            return pl.ds(base(slot), rows)
        return pl.ds(base(slot) + h * half_rows, half_rows)

    sums = {}

    def send_sum(c, k, slot_r, slot_l, h_r=None, h_l=None):
        def landing(ref, h):
            return ref.at[c, k] if h is None else ref.at[c, k, half_of(h)]

        sums["r", c, k] = (
            y.at[c, block(slot_r, h_r)],
            landing(from_prev, h_r),
            sum_r_send,
            sum_r_recv.at[c, k],
            nxt,
        )
        sums["l", c, k] = (
            y.at[c, block(slot_l, h_l)],
            landing(from_next, h_l),
            sum_l_send,
            sum_l_recv.at[c, k],
            prv,
        )

    def start_sum(key):
        sums[key] = go(remote(*sums[key]))

    def sum_start(c):
        send_sum(c, 0, half, half, 0, 1)
        start_sum(("r", c, 0))
        start_sum(("l", c, 0))

    def sum_step(c, k):
        send_sum(c, k, half + k, half - k)
        sums["r", c, k - 1].wait_recv()
        if k == 1:
            add(y.at[c, block(half + k, 0)], from_prev.at[c, 0, half_of(0)])
        else:
            add(y.at[c, block(half + k)], from_prev.at[c, k - 1])
        start_sum(("r", c, k))
        sums["l", c, k - 1].wait_recv()
        if k == 1:
            add(y.at[c, block(half - k, 1)], from_next.at[c, 0, half_of(1)])
        else:
            add(y.at[c, block(half - k)], from_next.at[c, k - 1])
        start_sum(("l", c, k))

    def sum_end(c):
        sums["r", c, half - 1].wait_recv()
        sums["l", c, half - 1].wait_recv()
        columns = slice(c * width, (c + 1) * width)
        out_stage[:, columns] = (
            y[c, block(0), :].astype(f32)
            + from_prev[c, half - 1].astype(f32)
            + from_next[c, half - 1].astype(f32)
        ).astype(bf16)
        outs.append(
            pltpu.make_async_copy(
                out_stage.at[:, pl.ds(c * width, width)],
                out_ref.at[:, pl.ds(c * width, width)],
                out_sem.at[c],
            )
        )
        outs[-1].start()

    everything = (0, 1)
    for i in range(4):
        local[i].wait()
        to_core[i].wait_recv()
    kv_step(1, 0)
    ring["f", 1, 1] = go(forward(1, 1))
    ring["b", 1, 0] = go(backward(1, 0))
    hidden(0, 2, everything, base(0), rows)
    make_queries_here()
    attend_slot(0)
    kv_step(1, 1)
    attend_slot(1)
    kv_step(2, 0)
    token_step(1, 0)
    attend_slot(count - 1)
    remote(coefs.at[1:], coefs.at[1:], coef_send, coef_recv, nxt).wait_recv()
    for slot in range(1, count):
        coefficient(slot)

    token_wait(1, 1)
    pair_norm(1)
    pass_on(0)
    hidden(0, 2, everything, base(1), tile_rows)
    kv_step(2, 1)
    token_pass(1, 1)
    attend_slot(2)
    kv_step(3, 0)
    attend_slot(count - 2)
    token_step(2, 0)
    pass_on(1)
    kv_step(3, 1)
    for i in range(2):
        relay[i].wait_recv()
    hidden(2, 4, (0,), base(0), rows)
    hidden(2, 4, (0,), base(1), tile_rows)
    attend_slot(3)
    attend_slot(count - 3)
    token_step(2, 1)
    pair_norm(2)
    hidden(0, 2, everything, base(2), tile_rows)
    kv_step(4, 0)
    kv_step(4, 1)
    pass_on(2)
    hidden(2, 4, (0,), base(2), tile_rows)
    token_step(3, 0)
    attend_slot(4)
    mix_start()
    token_step(3, 1)
    pair_norm(3)
    hidden(0, 2, everything, base(3), tile_rows)
    hidden(2, 4, (0,), base(3), tile_rows)
    pass_on(3)
    hidden(2, 3, (1,), base(1), tile_rows, half - 1)
    hidden(2, 3, (1,), base(0), rows)
    pass_on(4)
    for i in range(2, 4):
        relay[i].wait_recv()
    hidden(3, 4, (1,), base(1), tile_rows, half - 1)
    hidden(3, 4, (1,), base(0), rows)
    token_wait(half, 0)
    pass_on(5)
    norm(half)
    hidden(0, 4, everything, base(half), rows)

    passed = 2
    for kind, c, k in sum_plan(chunks, half):
        if kind == "down":
            down(c)
            if passed < chunks:
                pass_on(4 + passed)
                passed += 1
        elif kind == "step":
            sum_step(c, k)
        elif kind == "end":
            sum_end(c)
        elif kind == "cross":
            mix_cross()
        else:
            mix_end()

    ring_rows = half * rows - half_rows
    part_count = count - 1
    for ref, sem in (
        (kv_all.at[0:part_count, 0:rows], kvf_send),
        (kv_all.at[0:part_count, 0:rows], kvb_send),
        (kv_all.at[:, 0 : 2 * rows], kvc_send),
        (xn.at[0:ring_rows], fwd_send),
        (xn.at[0:ring_rows], bwd_send),
        (coefs.at[1:], coef_send),
        (xn.at[0 : 3 * ff], core_send),
        (xn.at[0 : 3 * ff], cross_send),
        (xn.at[0 : 3 * ff], relay_send),
        (y.at[:, 0:ring_rows], sum_r_send),
        (y.at[:, 0:ring_rows], sum_l_send),
    ):
        remote(ref, ref, sem, sem, nxt).wait_send()
    for copy in [kvr["x"], *q_copies, *mixes]:
        copy.wait_send()
    with jax.named_scope("outs"):
        for copy in outs:
            copy.wait()


def on_device_fused(
    q_latent,
    kv_latent,
    rope_key,
    q_gain,
    kv_gain,
    w_query,
    w_query_rot,
    w_key,
    w_value,
    w_mix_out,
    expert_input,
    ffn_gain,
    expert_ids,
    route_weights,
    w_gate_exp,
    w_up_exp,
    w_down_exp,
):
    count = lax.axis_size("ep")
    chunks = 8
    rows, depth = expert_input.shape
    ff = w_gate_exp.shape[2]
    heads = w_key.shape[1] // NOPE
    rank = kv_latent.shape[1]
    q_rank = q_latent.shape[1]
    group_rows = 4 * rows
    half = count // 2
    width = depth // chunks
    pieces = 4 + chunks
    head_lanes = heads * LANES
    kv_width = rank + LANES
    half_width = ROPE // 2
    frequency = np.float32(rope_base) ** (-np.arange(half_width, dtype=np.float32) / half_width)
    frequency = jnp.asarray(np.tile(frequency, LANES // half_width)[None, :], jnp.float32)
    bf16, f32 = jnp.bfloat16, jnp.float32
    dma = pltpu.SemaphoreType.DMA
    vmem = pl.BlockSpec(memory_space=pltpu.VMEM)
    hbm = pl.BlockSpec(memory_space=pl.ANY)
    return pl.pallas_call(
        functools.partial(layer_kernel, count, chunks),
        out_shape=[jax.ShapeDtypeStruct((rows, depth), bf16)] * 2,
        in_specs=[vmem] * 5 + [hbm] * 5 + [vmem, hbm, vmem, vmem, vmem] + [hbm] * 3,
        out_specs=[hbm, hbm],
        scratch_shapes=[
            pltpu.VMEM((rows, depth), bf16),
            pltpu.VMEM(w_query.shape, bf16),
            pltpu.VMEM(w_query_rot.shape, bf16),
            pltpu.VMEM(w_key.shape, bf16),
            pltpu.VMEM(w_value.shape, bf16),
            pltpu.VMEM(w_mix_out.shape, bf16),
            pltpu.VMEM((rows, depth), bf16),
            pltpu.VMEM((rows, depth), bf16),
            pltpu.VMEM((group_rows, LANES), f32),
            pltpu.VMEM((group_rows, LANES), f32),
            pltpu.VMEM((count, rows), f32),
            pltpu.VMEM((group_rows, q_rank), bf16),
            pltpu.VMEM((q_rank, 2 * head_lanes), bf16),
            pltpu.VMEM((group_rows, head_lanes), bf16),
            pltpu.VMEM((count, group_rows, kv_width), bf16),
            pltpu.VMEM((kv_width, head_lanes), bf16),
            pltpu.VMEM((heads * VR, kv_width), bf16),
            pltpu.VMEM((group_rows, head_lanes), bf16),
            pltpu.VMEM((heads, VR, group_rows), bf16),
            pltpu.VMEM((heads, 1, group_rows), f32),
            pltpu.VMEM((heads, VR, group_rows), f32),
            pltpu.VMEM((heads * VD, group_rows), bf16),
            pltpu.VMEM((4, rows, depth), bf16),
            pltpu.VMEM((2, rows, depth), bf16),
            pltpu.VMEM((rows, depth), bf16),
            pltpu.VMEM((count, rows, depth), bf16),
            pltpu.VMEM((count * rows, depth), bf16),
            pltpu.VMEM((4, 2, depth, ff), bf16),
            pltpu.VMEM((chunks, 4 * ff, width), bf16),
            pltpu.VMEM((count * rows, 4 * ff), bf16),
            pltpu.VMEM((chunks, count * rows, width), bf16),
            pltpu.VMEM((chunks, half, rows, width), bf16),
            pltpu.VMEM((chunks, half, rows, width), bf16),
            pltpu.VMEM((count, count, rows), f32),
            pltpu.VMEM((count * rows, 1), f32),
            dma((3,)),
            dma((3,)),
            dma((2,)),
            dma,
            dma((half, 2)),
            dma,
            dma((half, 2)),
            dma,
            dma((count, 2)),
            dma((3,)),
            dma((3,)),
            dma((6,)),
            dma((chunks + 1,)),
            dma((pieces,)),
            dma,
            dma,
            dma,
            dma((half, 2)),
            dma,
            dma((half, 2)),
            dma,
            dma((pieces,)),
            dma,
            dma((pieces,)),
            dma,
            dma((pieces,)),
            dma,
            dma((chunks, half)),
            dma,
            dma((chunks, half)),
        ],
        compiler_params=pltpu.CompilerParams(
            collective_id=0, has_side_effects=True, vmem_limit_bytes=63 * 1024 * 1024
        ),
        cost_estimate=pl.CostEstimate(
            flops=6 * count * rows * depth * 4 * ff,
            bytes_accessed=12 * depth * ff * 2,
            transcendentals=count * rows * 4 * ff,
        ),
        name="layer",
    )(
        q_latent,
        kv_latent,
        rope_key.T,
        q_gain.reshape(1, -1),
        kv_gain.reshape(1, -1),
        w_query,
        w_query_rot,
        w_key,
        w_value,
        w_mix_out,
        frequency,
        expert_input,
        ffn_gain.reshape(1, -1),
        expert_ids.T,
        route_weights.T,
        w_gate_exp,
        w_up_exp,
        w_down_exp,
    )


def fits(mesh):
    ep, tp = mesh.shape["ep"], mesh.shape["tp"]
    return tp == 4 and ep == 2 * tp


def solution(mesh):
    return jax.shard_map(
        on_device_fused if fits(mesh) else on_device_plain,
        mesh=mesh,
        in_specs=(
            P(("ep", "tp"), None),
            P(("ep", "tp"), None),
            P(("ep", "tp"), None),
            P(),
            P(),
            P(None, "tp"),
            P(None, "tp"),
            P(None, "tp"),
            P(None, "tp"),
            P("tp", None),
            P(("ep", "tp"), None),
            P(),
            P(("ep", "tp"), None),
            P(("ep", "tp"), None),
            P("ep", None, "tp"),
            P("ep", None, "tp"),
            P("ep", "tp", None),
        ),
        out_specs=(P(("ep", "tp"), None), P(("ep", "tp"), None)),
        check_vma=False,
    )
```

```python
import functools
import math

import jax
import jax.numpy as jnp
import numpy as np
from jax import lax
from jax.experimental import pallas as pl
from jax.experimental.pallas import tpu as pltpu
from jax.sharding import PartitionSpec as P

D = 2048
NOPE = 64
ROPE = 32
VD = 64
TOPK = 4
SEG = 64


norm_epsilon = 1e-06
rope_base = 10000.0
masked_score = -1e30


def rms_scale(values_in, gain_vec):
    floats = values_in.astype(jnp.float32)
    return (
        floats
        * lax.rsqrt(jnp.mean(floats * floats, axis=-1, keepdims=True) + norm_epsilon)
        * gain_vec
    )


def tables(positions):
    half_width = ROPE // 2
    frequency = rope_base ** (-jnp.arange(half_width, dtype=jnp.float32) / half_width)
    angles = positions.astype(jnp.float32)[:, None] * frequency[None, :]
    return (jnp.cos(angles), jnp.sin(angles))


def rotate_pairs(values_in, cosine, sine_table):
    half_width = values_in.shape[-1] // 2
    first, second = (values_in[..., :half_width], values_in[..., half_width:])
    return jnp.concatenate(
        [first * cosine - second * sine_table, first * sine_table + second * cosine], axis=-1
    )


LANES = 128


def pad_heads(weight, heads, width):
    split = weight.reshape(weight.shape[0], heads, width)
    return jnp.pad(split, ((0, 0), (0, 0), (0, LANES - width))).reshape(
        weight.shape[0], heads * LANES
    )


def make_queries(q_rows, q_gain, w_query, w_query_rot, heads, group_rows):
    start = lax.axis_index("ep") * group_rows
    cosine, sine_table = tables(start + jnp.arange(group_rows, dtype=jnp.int32))
    normed = rms_scale(q_rows, q_gain).astype(jnp.bfloat16)
    plain = jnp.dot(normed, w_query, preferred_element_type=jnp.float32).astype(jnp.bfloat16)
    turned = jnp.dot(normed, w_query_rot, preferred_element_type=jnp.float32).reshape(
        group_rows, heads, ROPE
    )
    turned = rotate_pairs(turned, cosine[:, None, :], sine_table[:, None, :]).astype(jnp.bfloat16)
    blank = jnp.zeros((group_rows, heads, LANES - NOPE - ROPE), jnp.bfloat16)
    joined = jnp.concatenate([plain.reshape(group_rows, heads, NOPE), turned, blank], axis=-1)
    return joined.reshape(group_rows, heads * LANES)


def make_keys(kv_rows, kv_gain, w_key, w_value, heads):
    row_count = kv_rows.shape[0]
    rank = w_key.shape[0]
    normed = rms_scale(kv_rows[:, :rank], kv_gain).astype(jnp.bfloat16)
    cosine, sine_table = tables(jnp.arange(row_count, dtype=jnp.int32))
    turned = rotate_pairs(kv_rows[:, rank:].astype(jnp.float32), cosine, sine_table)
    turned = jnp.pad(
        turned.astype(jnp.bfloat16), ((0, 0), (NOPE, LANES - NOPE - ROPE))
    )
    plain = jnp.dot(normed, pad_heads(w_key, heads, NOPE), preferred_element_type=jnp.float32)
    keys = plain.astype(jnp.bfloat16) + jnp.tile(turned, (1, heads))
    raw = jnp.dot(normed, pad_heads(w_value, heads, VD), preferred_element_type=jnp.float32)
    ones = (jnp.arange(heads * LANES, dtype=jnp.int32) % LANES == VD).astype(jnp.bfloat16)
    return keys, raw.astype(jnp.bfloat16) + ones[None, :]


def attention_kernel(heads, chunk, group_ref, q_ref, k_ref, v_ref, o_ref, max_ref, acc_ref):
    step = pl.program_id(0)
    group = group_ref[0]
    rows = q_ref.shape[0]
    keys = k_ref.shape[0]
    log_scale = (NOPE + ROPE) ** (-0.5) * math.log2(math.e)

    @pl.when(step == 0)
    def _():
        max_ref[...] = jnp.full(max_ref.shape, masked_score, jnp.float32)
        acc_ref[...] = jnp.zeros(acc_ref.shape, jnp.float32)

    def work(masked):
        for head in range(heads):
            lanes = slice(head * LANES, (head + 1) * LANES)
            for first in range(0, rows, chunk):
                part = slice(first, first + chunk)
                scores = lax.dot_general(
                    q_ref[part, lanes],
                    k_ref[:, lanes],
                    (((1,), (1,)), ((), ())),
                    preferred_element_type=jnp.float32,
                )
                if masked:
                    row_id = lax.broadcasted_iota(jnp.int32, (chunk, keys), 0) + first
                    col_id = lax.broadcasted_iota(jnp.int32, (chunk, keys), 1)
                    scores = jnp.where(col_id // SEG <= row_id // SEG, scores, masked_score)
                old = max_ref[head, part, :]
                new = jnp.maximum(old, jnp.max(scores, axis=-1, keepdims=True))
                weights = jnp.exp2((scores - new[:, :1]) * log_scale).astype(jnp.bfloat16)
                factor = jnp.exp2((old - new) * log_scale)
                max_ref[head, part, :] = new
                acc_ref[head, part, :] = acc_ref[head, part, :] * factor + jnp.dot(
                    weights, v_ref[:, lanes], preferred_element_type=jnp.float32
                )

    @pl.when(step < group)
    def _():
        work(False)

    @pl.when(step == group)
    def _():
        work(True)

    @pl.when(step == pl.num_programs(0) - 1)
    def _():
        for head in range(heads):
            acc = acc_ref[head]
            o_ref[:, head * VD : (head + 1) * VD] = (
                acc[:, :VD] / acc[:, VD : VD + 1]
            ).astype(jnp.bfloat16)


def attend(queries, keys, values, heads, group_rows):
    group = lax.axis_index("ep").astype(jnp.int32).reshape(1)
    blocks = keys.shape[0] // group_rows
    width = heads * LANES
    chunk = 256 if group_rows % 256 == 0 else group_rows
    return pl.pallas_call(
        functools.partial(attention_kernel, heads, chunk),
        out_shape=jax.ShapeDtypeStruct((group_rows, heads * VD), jnp.bfloat16),
        grid_spec=pltpu.PrefetchScalarGridSpec(
            num_scalar_prefetch=1,
            grid=(blocks,),
            in_specs=[
                pl.BlockSpec((group_rows, width), lambda i, g: (0, 0)),
                pl.BlockSpec((group_rows, width), lambda i, g: (jnp.minimum(i, g[0]), 0)),
                pl.BlockSpec((group_rows, width), lambda i, g: (jnp.minimum(i, g[0]), 0)),
            ],
            out_specs=pl.BlockSpec((group_rows, heads * VD), lambda i, g: (0, 0)),
            scratch_shapes=[
                pltpu.VMEM((heads, group_rows, LANES), jnp.float32),
                pltpu.VMEM((heads, group_rows, LANES), jnp.float32),
            ],
        ),
        compiler_params=pltpu.CompilerParams(
            dimension_semantics=("arbitrary",), vmem_limit_bytes=24 * 1024 * 1024
        ),
        cost_estimate=pl.CostEstimate(
            flops=4 * heads * group_rows * keys.shape[0] * LANES * 2,
            bytes_accessed=4 * keys.shape[0] * width,
            transcendentals=heads * group_rows * keys.shape[0],
        ),
        name="attend",
    )(group, queries, keys, values)


def on_device_plain(
    q_latent,
    kv_latent,
    rope_key,
    q_gain,
    kv_gain,
    w_query,
    w_query_rot,
    w_key,
    w_value,
    w_mix_out,
    expert_input,
    ffn_gain,
    expert_ids,
    route_weights,
    w_gate_exp,
    w_up_exp,
    w_down_exp,
):
    tok_rows = q_latent.shape[0]
    tp_count = lax.axis_size("tp")
    expert_count = lax.axis_size("ep")
    slot_count = 3 * tok_rows * TOPK // (2 * expert_count)
    group_rows = tp_count * tok_rows
    heads_here = w_key.shape[1] // NOPE

    gate_all = lax.all_gather(w_gate_exp[0], "tp", axis=0)
    up_all = lax.all_gather(w_up_exp[0], "tp", axis=0)
    down_all = lax.all_gather(w_down_exp[0], "tp", axis=0)

    normed = rms_scale(expert_input, ffn_gain).astype(jnp.bfloat16)
    routed = expert_ids.reshape(-1)
    onehot = (routed[:, None] == jnp.arange(expert_count, dtype=jnp.int32)[None, :]).astype(
        jnp.int32
    )
    slot_number = jnp.sum((jnp.cumsum(onehot, axis=0) - 1) * onehot, axis=-1)
    slot_place = (routed * slot_count + slot_number).reshape(tok_rows, TOPK)
    slot_line = jnp.arange(expert_count * slot_count, dtype=jnp.int32)
    picks = [
        (slot_place[:, route_rank][:, None] == slot_line[None, :]).astype(jnp.bfloat16)
        for route_rank in range(TOPK)
    ]
    dispatch = picks[0]
    for route_rank in range(1, TOPK):
        dispatch = dispatch + picks[route_rank]
    outgoing = lax.dot_general(
        dispatch, normed, (((0,), (0,)), ((), ())), preferred_element_type=jnp.float32
    ).astype(jnp.bfloat16)
    arrived = lax.all_to_all(
        outgoing.reshape(expert_count, slot_count, D), "ep", split_axis=0, concat_axis=0, tiled=True
    )
    rows = arrived.reshape(expert_count * slot_count, D)

    own_rows = jnp.concatenate([kv_latent, rope_key], axis=1)
    ep_rows = lax.all_gather(own_rows, "ep", axis=0, tiled=True)
    column_count = own_rows.shape[1]
    piece_width = column_count // 3 if column_count % 3 == 0 else column_count
    pieces = [
        lax.all_gather(ep_rows[:, first : first + piece_width], "tp", axis=0)
        for first in range(0, column_count, piece_width)
    ]
    kv_rows = (
        jnp.concatenate(pieces, axis=2)
        .reshape(tp_count, expert_count, tok_rows, column_count)
        .transpose(1, 0, 2, 3)
        .reshape(expert_count * group_rows, column_count)
    )
    q_rows = lax.all_gather(q_latent, "tp", axis=0, tiled=True)
    queries = make_queries(q_rows, q_gain, w_query, w_query_rot, heads_here, group_rows)
    keys, values = make_keys(kv_rows, kv_gain, w_key, w_value, heads_here)
    attention = attend(queries, keys, values, heads_here, group_rows)

    total = jnp.zeros((rows.shape[0], D), jnp.float32)
    for block in range(tp_count):
        gate_part = jnp.dot(rows, gate_all[block], preferred_element_type=jnp.float32)
        up_part = jnp.dot(rows, up_all[block], preferred_element_type=jnp.float32)
        hidden = (jax.nn.silu(gate_part) * up_part).astype(jnp.bfloat16)
        part = jnp.dot(hidden, down_all[block], preferred_element_type=jnp.float32)
        total = total + part.astype(jnp.bfloat16).astype(jnp.float32)
    summed = total.astype(jnp.bfloat16)
    results = lax.all_to_all(
        summed.reshape(expert_count, slot_count, D), "ep", split_axis=0, concat_axis=0, tiled=True
    ).reshape(expert_count * slot_count, D)

    partial_out = jnp.dot(attention, w_mix_out, preferred_element_type=jnp.float32).astype(
        jnp.bfloat16
    )
    mixer_out = lax.psum_scatter(partial_out, "tp", scatter_dimension=0, tiled=True)

    fetched = jnp.dot(
        jnp.concatenate(picks, axis=0), results, preferred_element_type=jnp.float32
    ).astype(jnp.bfloat16)
    combined = jnp.zeros((tok_rows, D), jnp.float32)
    for route_rank in range(TOPK):
        piece = fetched[route_rank * tok_rows : (route_rank + 1) * tok_rows].astype(jnp.float32)
        combined = combined + route_weights[:, route_rank : route_rank + 1] * piece
    return (mixer_out, combined.astype(jnp.bfloat16))


MESH = pl.DeviceIdType.MESH
VR = VD + 16


def ring_place(index, count):
    side = index % 2
    line = index // 2
    return line + side * (count - 1 - 2 * line)


def ring_index(place, count):
    side = place // (count // 2)
    line = place + side * (count - 1 - 2 * place)
    return 2 * line + side


def remote(src, dst, send, recv, device):
    return pltpu.make_async_remote_copy(
        src_ref=src, dst_ref=dst, send_sem=send, recv_sem=recv, device_id=device, device_id_type=MESH
    )


def sum_plan(chunks, half):
    block = 11.2 / chunks
    lag = 1.7
    now, link = 0.0, 0.0
    arrive, plan = {}, []
    downs, side = 0, [("cross", 12.0), ("close", 34.0)]
    while downs < chunks or arrive or side:
        ready = sorted((k, c) for (c, k), at in arrive.items() if at <= now)
        can_down = downs < chunks and downs * 22.4 / chunks <= now
        if side and side[0][1] <= now:
            plan.append((side.pop(0)[0], 0, 0))
        elif can_down and (link > now + 0.4 or not ready):
            plan.append(("down", downs, 0))
            link = max(link, now + 0.4) + block / 2
            arrive[downs, 1] = link + lag
            now += 10.0 / chunks
            downs += 1
        elif ready:
            k, c = ready[0]
            del arrive[c, k]
            now += 0.1
            if k < half:
                plan.append(("step", c, k))
                link = max(link, now) + block
                arrive[c, k + 1] = link + lag
            else:
                plan.append(("end", c, k))
        else:
            times = list(arrive.values()) + [at for _, at in side]
            if downs < chunks:
                times.append(downs * 22.4 / chunks)
            now = max(now + 0.01, min(times))
    return plan


def layer_kernel(
    count,
    chunks,
    q_ref,
    kv_ref,
    rope_ref,
    q_gain_ref,
    kv_gain_ref,
    w_query_ref,
    w_rot_ref,
    w_key_ref,
    w_value_ref,
    w_mix_ref,
    freq_ref,
    x_ref,
    gain_ref,
    ids_ref,
    route_ref,
    gate_ref,
    up_ref,
    down_ref,
    both_out_ref,
    x_now,
    w_query_now,
    w_rot_now,
    w_key_now,
    w_value_now,
    w_mix_now,
    mix_stage,
    out_stage,
    cos_ref,
    sin_ref,
    coef_ref,
    q_all,
    wq_cat,
    queries,
    kv_all,
    w_kv,
    w_vt,
    k_now,
    v_now,
    row_max,
    row_acc,
    attended,
    mixed,
    from_core,
    from_cross,
    raw,
    xn,
    wgu,
    wd,
    hid,
    y,
    from_prev,
    from_next,
    coefs,
    coef_col,
    q_send,
    q_recv,
    kvx_sem,
    kvf_send,
    kvf_recv,
    kvb_send,
    kvb_recv,
    kvc_send,
    kvc_recv,
    mix_send,
    mix_recv,
    in_sem,
    out_sem,
    local_sem,
    coef_send,
    coef_recv,
    fwd_send,
    fwd_recv,
    bwd_send,
    bwd_recv,
    core_send,
    core_recv,
    cross_send,
    cross_recv,
    relay_send,
    relay_recv,
    sum_r_send,
    sum_r_recv,
    sum_l_send,
    sum_l_recv,
):
    bf16, f32 = jnp.bfloat16, jnp.float32
    mix_out_ref, out_ref = both_out_ref.at[0], both_out_ref.at[1]
    rows = x_ref.shape[0]
    half_rows = rows // 2
    half = count // 2
    ff = gate_ref.shape[2]
    fh = ff // 2
    width = x_ref.shape[1] // chunks
    group_rows = 4 * rows
    heads = w_key_ref.shape[1] // NOPE
    rank = kv_ref.shape[1]
    head_lanes = heads * LANES
    me = lax.axis_index("ep")
    tp = lax.axis_index("tp")
    place = ring_place(me, count)
    nxt = (ring_index((place + 1) % count, count), tp)
    prv = (ring_index((place + count - 1) % count, count), tp)
    core_peer = (me, tp + 1 - 2 * (tp % 2))
    cross_peer = (me, (tp + 2) % 4)

    barrier = pltpu.get_barrier_semaphore()
    for step in range(1, count):
        pl.semaphore_signal(
            barrier,
            inc=1,
            device_id=(ring_index((place + step) % count, count), tp),
            device_id_type=MESH,
        )
    for peer in (core_peer, cross_peer):
        pl.semaphore_signal(barrier, inc=1, device_id=peer, device_id_type=MESH)

    inputs = []
    for i, (src, dst) in enumerate(
        (
            (x_ref, x_now),
            (w_key_ref, w_key_now),
            (w_value_ref, w_value_now),
            (w_query_ref, w_query_now),
            (w_rot_ref, w_rot_now),
            (w_mix_ref, w_mix_now),
        )
    ):
        inputs.append(pltpu.make_async_copy(src, dst, in_sem.at[i]))
        inputs[-1].start()

    def go(copy):
        copy.start()
        return copy

    def half_of(h):
        return pl.ds(h * half_rows, half_rows)

    def forward(step, h):
        src = x_ref.at[half_of(h)] if step == 1 else raw.at[step - 1, half_of(h)]
        return remote(
            src, raw.at[step, half_of(h)], fwd_send, fwd_recv.at[step - 1, h], nxt
        )

    def backward(step, h):
        src = x_ref.at[half_of(h)] if step == 1 else raw.at[count - step + 1, half_of(h)]
        return remote(
            src, raw.at[count - step, half_of(h)], bwd_send, bwd_recv.at[step - 1, h], prv
        )

    pl.semaphore_wait(barrier, count + 1)
    ring = {}
    ring["f", 1, 0] = go(forward(1, 0))
    ring["b", 1, 1] = go(backward(1, 1))

    def rows_of(index):
        return pl.ds(pl.multiple_of(index * rows, rows), rows)

    own_rows, cross_rows = rows_of(tp), rows_of((tp + 2) % 4)

    def scaled(ref, gain):
        floats = ref[...].astype(f32)
        scale = lax.rsqrt(jnp.mean(floats * floats, axis=-1, keepdims=True) + norm_epsilon)
        return (floats * scale * gain[...]).astype(bf16)

    def turn_table(first, size):
        lane = lax.broadcasted_iota(jnp.int32, (size, LANES), 1)
        row = lax.broadcasted_iota(jnp.int32, (size, LANES), 0)
        angle = (me * group_rows + first + row).astype(f32) * freq_ref[...]
        inside = (lane >= NOPE) & (lane < NOPE + ROPE)
        sine = jnp.where(inside, jnp.sin(angle), 0.0)
        return (
            jnp.where(inside, jnp.cos(angle), jnp.where(lane < NOPE, 1.0, 0.0)),
            jnp.where(lane < NOPE + ROPE // 2, -sine, sine),
        )

    turn_row = lax.broadcasted_iota(jnp.int32, (ROPE, LANES), 0)
    turn_col = lax.broadcasted_iota(jnp.int32, (ROPE, LANES), 1) - NOPE
    straight = (turn_row == turn_col).astype(f32).astype(bf16)
    swapped = (
        ((turn_row == turn_col + ROPE // 2) & (turn_col < ROPE // 2))
        | ((turn_row == turn_col - ROPE // 2) & (turn_col >= ROPE // 2))
    )
    swapped = jnp.where(swapped, 1.0, 0.0).astype(bf16)
    rope = rope_ref[...]
    own_cos, own_sin = turn_table(tp * rows, rows)
    by_column = (((0,), (0,)), ((), ()))
    turned = (
        lax.dot_general(rope, straight, by_column, preferred_element_type=f32) * own_cos
        + lax.dot_general(rope, swapped, by_column, preferred_element_type=f32) * own_sin
    )
    lane = lax.broadcasted_iota(jnp.int32, (rows, LANES), 1)
    kv_all[0, own_rows, 0:rank] = scaled(kv_ref, kv_gain_ref)
    kv_all[0, own_rows, rank : rank + LANES] = jnp.where(
        lane == NOPE + ROPE, 1.0, turned
    ).astype(bf16)
    q_all[own_rows, :] = scaled(q_ref, q_gain_ref)
    expert_id = lax.broadcasted_iota(jnp.int32, (count, rows), 0)
    coef = jnp.zeros((count, rows), f32)
    for k in range(TOPK):
        coef += jnp.where(ids_ref[k : k + 1, :] == expert_id, route_ref[k : k + 1, :], 0.0)
    coef_ref[...] = coef

    part_rows = (own_rows, cross_rows)

    def kv_forward(step, p):
        return remote(
            kv_all.at[step - 1, part_rows[p]],
            kv_all.at[step, part_rows[p]],
            kvf_send,
            kvf_recv.at[step - 1, p],
            nxt,
        )

    def kv_backward(step, p):
        return remote(
            kv_all.at[(count - step + 1) % count, part_rows[p]],
            kv_all.at[count - step, part_rows[p]],
            kvb_send,
            kvb_recv.at[step - 1, p],
            prv,
        )

    def kv_core(slot, p):
        return remote(
            kv_all.at[slot, part_rows[p]],
            kv_all.at[slot, part_rows[p]],
            kvc_send,
            kvc_recv.at[slot, p],
            core_peer,
        )

    def piece(i, slot):
        if i < 4:
            return wgu.at[slot, i // 2, i % 2]
        return wd.at[i - 4, pl.ds(slot * ff, ff)]

    def own_piece(i):
        if i < 4:
            ref = (gate_ref, up_ref)[i % 2]
            return ref.at[0, :, pl.ds((i // 2) * fh, fh)]
        return down_ref.at[0, :, pl.ds((i - 4) * width, width)]

    kvr = {}
    kvr["x"] = go(
        remote(
            kv_all.at[0, own_rows],
            kv_all.at[0, own_rows],
            kvx_sem.at[0],
            kvx_sem.at[1],
            cross_peer,
        )
    )
    kvr["f", 1, 0] = go(kv_forward(1, 0))
    kvr["b", 1, 0] = go(kv_backward(1, 0))
    kvr["c", 0, 0] = go(kv_core(0, 0))
    q_copies = [
        go(remote(q_all.at[own_rows], q_all.at[own_rows], q_send.at[i], q_recv.at[i], peer))
        for i, peer in enumerate((core_peer, cross_peer))
    ]
    to_coefs = [
        go(
            remote(
                coef_ref,
                coefs.at[step],
                coef_send,
                coef_recv,
                (ring_index((place + step) % count, count), tp),
            )
        )
        for step in range(1, count)
    ]
    local, to_core, to_cross, relay = [], [], [], []
    for i in range(4 + chunks):
        to_cross.append(
            go(remote(own_piece(i), piece(i, 2), cross_send, cross_recv.at[i], cross_peer))
        )
        to_core.append(
            go(remote(own_piece(i), piece(i, 1), core_send, core_recv.at[i], core_peer))
        )
        copy = pltpu.make_async_copy(own_piece(i), piece(i, 0), local_sem.at[i])
        copy.start()
        local.append(copy)

    def pass_on(i):
        to_cross[i].wait_recv()
        relay.append(
            go(remote(piece(i, 2), piece(i, 3), relay_send, relay_recv.at[i], core_peer))
        )

    order = [0, half]
    for step in range(1, half):
        order += [step, count - step]

    def base(slot):
        return order.index(slot) * rows

    def norm(slot):
        xn[base(slot) : base(slot) + rows, :] = scaled(
            x_now if slot == 0 else raw.at[slot], gain_ref
        )

    def coefficient(slot):
        source = coef_ref if slot == 0 else coefs.at[slot]
        line = jnp.broadcast_to(source[pl.ds(me, 1), :], (rows, rows))
        row_id = lax.broadcasted_iota(jnp.int32, (rows, rows), 0)
        col_id = lax.broadcasted_iota(jnp.int32, (rows, rows), 1)
        coef_col[base(slot) : base(slot) + rows, :] = jnp.sum(
            jnp.where(row_id == col_id, line, 0.0), axis=-1, keepdims=True
        )

    w_kv[...] = jnp.zeros_like(w_kv)
    inputs[1].wait()
    for head in range(heads):
        at = head * LANES
        w_kv[0:rank, at : at + NOPE] = w_key_now[:, head * NOPE : (head + 1) * NOPE]
    pass_row = lax.broadcasted_iota(jnp.int32, (LANES, head_lanes), 0)
    pass_col = lax.broadcasted_iota(jnp.int32, (LANES, head_lanes), 1)
    as_key = (
        (pass_col % LANES == pass_row) & (pass_row >= NOPE) & (pass_row < NOPE + ROPE)
    )
    w_kv[rank : rank + LANES, :] = jnp.where(as_key, 1.0, 0.0).astype(bf16)

    kvr["x"].wait_recv()
    kvr["f", 1, 1] = go(kv_forward(1, 1))
    kvr["b", 1, 1] = go(kv_backward(1, 1))
    kvr["c", 0, 1] = go(kv_core(0, 1))
    ring["f", 1, 1] = go(forward(1, 1))
    ring["b", 1, 0] = go(backward(1, 0))

    cos_ref[...], sin_ref[...] = turn_table(0, group_rows)
    wq_cat[...] = jnp.zeros_like(wq_cat)
    inputs[3].wait()
    inputs[4].wait()
    for head in range(heads):
        at = head * LANES
        turn = head * ROPE
        wq_cat[:, at : at + NOPE] = w_query_now[:, head * NOPE : (head + 1) * NOPE]
        wq_cat[:, at + NOPE : at + NOPE + ROPE] = w_rot_now[:, turn : turn + ROPE]
        at += head_lanes + NOPE
        wq_cat[:, at : at + ROPE // 2] = w_rot_now[:, turn + ROPE // 2 : turn + ROPE]
        wq_cat[:, at + ROPE // 2 : at + ROPE] = w_rot_now[:, turn : turn + ROPE // 2]

    inputs[2].wait()
    flipped = jnp.transpose(w_value_now[...].astype(f32)).astype(bf16)
    one_row = lax.broadcasted_iota(jnp.int32, (VR, rank + LANES), 0)
    one_col = lax.broadcasted_iota(jnp.int32, (VR, rank + LANES), 1)
    ones = ((one_row == VD) & (one_col == rank + NOPE + ROPE)).astype(f32).astype(bf16)
    for head in range(heads):
        w_vt[head * VR : (head + 1) * VR, :] = ones
        w_vt[head * VR : head * VR + VD, 0:rank] = flipped[head * VD : (head + 1) * VD, :]
    inputs[0].wait()
    norm(0)
    coefficient(0)
    row_max[...] = jnp.full(row_max.shape, masked_score, f32)
    row_acc[...] = jnp.zeros(row_acc.shape, f32)
    q_copies[1].wait_recv()
    q_copies.append(
        go(
            remote(
                q_all.at[cross_rows], q_all.at[cross_rows], q_send.at[2], q_recv.at[2], core_peer
            )
        )
    )

    def make_queries_here():
        q_copies[0].wait_recv()
        q_copies[2].wait_recv()
        both = jnp.dot(q_all[...], wq_cat[...], preferred_element_type=f32)
        for head in range(heads):
            at = head * LANES
            queries[:, at : at + LANES] = (
                both[:, at : at + LANES] * cos_ref[...]
                + both[:, head_lanes + at : head_lanes + at + LANES] * sin_ref[...]
            ).astype(bf16)

    log_scale = (NOPE + ROPE) ** (-0.5) * math.log2(math.e)

    def work(slot, masked):
        k_now[...] = jnp.dot(kv_all[slot], w_kv[...], preferred_element_type=f32).astype(bf16)
        turned_values = lax.dot_general(
            w_vt[...], kv_all[slot], (((1,), (1,)), ((), ())), preferred_element_type=f32
        )
        v_now[...] = turned_values.astype(bf16).reshape(heads, VR, group_rows)

        @pl.loop(0, heads // 2)
        def _(pair):
            for sub in range(2):
                head = pair * 2 + sub
                lanes = pl.ds(pl.multiple_of(head * LANES, LANES), LANES)
                scores = lax.dot_general(
                    k_now[:, lanes],
                    queries[:, lanes],
                    (((1,), (1,)), ((), ())),
                    preferred_element_type=f32,
                )
                if masked:
                    key_id = lax.broadcasted_iota(jnp.int32, scores.shape, 0)
                    query_id = lax.broadcasted_iota(jnp.int32, scores.shape, 1)
                    scores = jnp.where(key_id // SEG <= query_id // SEG, scores, masked_score)
                old = row_max[head]
                new = jnp.maximum(old, jnp.max(scores, axis=0, keepdims=True))
                weights = jnp.exp2((scores - new) * log_scale).astype(bf16)
                factor = jnp.exp2((old - new) * log_scale)
                row_max[head] = new
                row_acc[head] = row_acc[head] * factor + jnp.dot(
                    v_now[head], weights, preferred_element_type=f32
                )

    def attend_slot(slot):
        kvr["c", slot, 0].wait_recv()
        kvr["c", slot, 1].wait_recv()
        if slot == 0:
            work(0, True)
        else:

            @pl.when(ring_index((place + count - slot) % count, count) < me)
            def _():
                work(slot, False)

    def kv_step(step, p):
        if step < half or p == 0:
            kvr["f", step, p].wait_recv()
            if step + 1 < half or (step + 1 == half and p == 0):
                kvr["f", step + 1, p] = go(kv_forward(step + 1, p))
            kvr["c", step, p] = go(kv_core(step, p))
        if step < half or p == 1:
            kvr["b", step, p].wait_recv()
            if step + 1 < half or (step + 1 == half and p == 1):
                kvr["b", step + 1, p] = go(kv_backward(step + 1, p))
            kvr["c", count - step, p] = go(kv_core(count - step, p))

    def token_wait(step, i):
        ring["f", step, i].wait_recv()
        ring["b", step, 1 - i].wait_recv()

    def token_pass(step, i):
        if step + 1 < half or i == 0:
            ring["f", step + 1, i] = go(forward(step + 1, i))
            ring["b", step + 1, 1 - i] = go(backward(step + 1, 1 - i))

    def token_step(step, i):
        token_wait(step, i)
        token_pass(step, i)

    tile_rows = 2 * rows

    def hidden(slot_from, slot_to, halves, first, size, tiles=1):
        @pl.loop(slot_from, slot_to)
        def _(slot):
            @pl.loop(0, tiles)
            def _(tile):
                part = pl.ds(pl.multiple_of(first + tile * size, rows), size)
                for h in halves:
                    weight = jnp.concatenate([wgu[slot, h, 0], wgu[slot, h, 1]], axis=1)
                    both = jnp.dot(xn[part, :], weight, preferred_element_type=f32)
                    gate = both[:, :fh]
                    at = pl.ds(pl.multiple_of((slot * 2 + h) * fh, fh), fh)
                    hid[part, at] = (gate * jax.nn.sigmoid(gate) * both[:, fh:]).astype(bf16)

    def pair_norm(step):
        norm(step)
        norm(count - step)

    def pair_first(step):
        return base(step)

    mixes = []

    def mix_start():
        for head in range(heads):
            acc = row_acc[head]
            attended[head * VD : (head + 1) * VD, :] = (
                acc[:VD, :] / acc[VD : VD + 1, :]
            ).astype(bf16)
        inputs[5].wait()

        @pl.loop(0, 4)
        def _(block):
            part = pl.ds(pl.multiple_of(block * rows, rows), rows)
            mixed[block] = lax.dot_general(
                attended[:, part], w_mix_now[...], by_column, preferred_element_type=f32
            ).astype(bf16)

        for i, index in enumerate((3 - tp, tp + 1 - 2 * (tp % 2))):
            mixes.append(
                go(
                    remote(
                        mixed.at[index], from_core.at[i], mix_send.at[i], mix_recv.at[i], core_peer
                    )
                )
            )

    def add(target, source):
        target[...] = (target[...].astype(f32) + source[...].astype(f32)).astype(bf16)

    def mix_cross():
        mixes[0].wait_recv()
        add(mixed.at[(tp + 2) % 4], from_core.at[0])
        mixes.append(
            go(
                remote(
                    mixed.at[(tp + 2) % 4], from_cross, mix_send.at[2], mix_recv.at[2], cross_peer
                )
            )
        )

    outs = []

    def mix_end():
        mixes[1].wait_recv()
        mixes[2].wait_recv()
        mix_stage[...] = (
            mixed[tp].astype(f32) + from_core[1].astype(f32) + from_cross[...].astype(f32)
        ).astype(bf16)
        outs.append(pltpu.make_async_copy(mix_stage, mix_out_ref, out_sem.at[chunks]))
        outs[-1].start()

    def down_tile(c, pair):
        part = pl.ds(pl.multiple_of(pair * tile_rows, tile_rows), tile_rows)
        acc = jnp.dot(hid[part, :], wd[c], preferred_element_type=f32)
        y[c, part, :] = (acc * coef_col[part, :]).astype(bf16)

    def down_head(c):
        local[4 + c].wait()
        to_core[4 + c].wait_recv()
        relay[4 + c].wait_recv()
        down_tile(c, 0)
        sum_start(c)

    def down_rest(c):
        @pl.loop(1, half)
        def _(back):
            down_tile(c, half - back)

    def down(c):
        down_head(c)
        down_rest(c)

    def block(slot, h=None):
        if h is None:
            return pl.ds(base(slot), rows)
        return pl.ds(base(slot) + h * half_rows, half_rows)

    sums = {}

    def send_sum(c, k, slot_r, slot_l, h_r=None, h_l=None):
        def landing(ref, h):
            return ref.at[c, k] if h is None else ref.at[c, k, half_of(h)]

        sums["r", c, k] = (
            y.at[c, block(slot_r, h_r)],
            landing(from_prev, h_r),
            sum_r_send,
            sum_r_recv.at[c, k],
            nxt,
        )
        sums["l", c, k] = (
            y.at[c, block(slot_l, h_l)],
            landing(from_next, h_l),
            sum_l_send,
            sum_l_recv.at[c, k],
            prv,
        )

    def start_sum(key):
        sums[key] = go(remote(*sums[key]))

    def sum_start(c):
        send_sum(c, 0, half, half, 0, 1)
        start_sum(("r", c, 0))
        start_sum(("l", c, 0))

    def sum_step(c, k):
        send_sum(c, k, half + k, half - k)
        sums["r", c, k - 1].wait_recv()
        if k == 1:
            add(y.at[c, block(half + k, 0)], from_prev.at[c, 0, half_of(0)])
        else:
            add(y.at[c, block(half + k)], from_prev.at[c, k - 1])
        start_sum(("r", c, k))
        sums["l", c, k - 1].wait_recv()
        if k == 1:
            add(y.at[c, block(half - k, 1)], from_next.at[c, 0, half_of(1)])
        else:
            add(y.at[c, block(half - k)], from_next.at[c, k - 1])
        start_sum(("l", c, k))

    def sum_end(c):
        sums["r", c, half - 1].wait_recv()
        sums["l", c, half - 1].wait_recv()
        columns = slice(c * width, (c + 1) * width)
        out_stage[:, columns] = (
            y[c, block(0), :].astype(f32)
            + from_prev[c, half - 1].astype(f32)
            + from_next[c, half - 1].astype(f32)
        ).astype(bf16)
        outs.append(
            pltpu.make_async_copy(
                out_stage.at[:, pl.ds(c * width, width)],
                out_ref.at[:, pl.ds(c * width, width)],
                out_sem.at[c],
            )
        )
        outs[-1].start()

    everything = (0, 1)
    for i in range(4):
        local[i].wait()
        to_core[i].wait_recv()
    hidden(0, 2, everything, base(0), rows)
    kv_step(1, 0)
    make_queries_here()
    kv_step(1, 1)
    token_step(1, 0)
    attend_slot(0)
    attend_slot(1)
    remote(coefs.at[1:], coefs.at[1:], coef_send, coef_recv, nxt).wait_recv()
    for slot in range(1, count):
        coefficient(slot)
    attend_slot(count - 1)

    kv_step(2, 0)
    pass_on(0)
    token_wait(1, 1)
    pair_norm(1)
    kv_step(2, 1)
    token_pass(1, 1)
    hidden(0, 2, everything, base(1), tile_rows)
    attend_slot(2)
    attend_slot(count - 2)
    token_wait(2, 0)
    kv_step(3, 0)
    pass_on(1)
    kv_step(3, 1)
    token_pass(2, 0)
    for i in range(2):
        relay[i].wait_recv()
    hidden(2, 4, (0,), base(0), rows)
    hidden(2, 4, (0,), base(1), tile_rows)
    attend_slot(3)
    attend_slot(count - 3)
    token_step(2, 1)
    kv_step(4, 0)
    kv_step(4, 1)
    pair_norm(2)
    hidden(0, 2, everything, base(2), tile_rows)
    pass_on(2)
    hidden(2, 4, (0,), base(2), tile_rows)
    attend_slot(4)
    token_step(3, 0)
    mix_start()
    token_wait(3, 1)
    pair_norm(3)
    hidden(0, 2, everything, base(3), tile_rows)
    pass_on(3)
    hidden(2, 4, (0,), base(3), tile_rows)
    hidden(2, 3, (1,), base(1), tile_rows, half - 1)
    hidden(2, 3, (1,), base(0), rows)
    pass_on(4)
    token_wait(half, 0)
    norm(half)
    hidden(0, 3, everything, base(half), rows)
    for i in range(2, 4):
        relay[i].wait_recv()
    hidden(3, 4, everything, base(half), rows)
    hidden(3, 4, (1,), base(0), rows)
    down_head(0)
    pass_on(5)
    hidden(3, 4, (1,), base(1), tile_rows, half - 1)
    down_rest(0)

    passed = 2
    for kind, c, k in sum_plan(chunks, half):
        if kind == "down":
            if c > 0:
                down(c)
            if passed < chunks:
                pass_on(4 + passed)
                passed += 1
        elif kind == "step":
            sum_step(c, k)
        elif kind == "end":
            sum_end(c)
        elif kind == "cross":
            mix_cross()
        else:
            mix_end()

    ring_rows = half * rows - half_rows
    part_count = count - 1
    for ref, sem in (
        (kv_all.at[0:part_count, 0:rows], kvf_send),
        (kv_all.at[0:part_count, 0:rows], kvb_send),
        (kv_all.at[:, 0 : 2 * rows], kvc_send),
        (xn.at[0:ring_rows], fwd_send),
        (xn.at[0:ring_rows], bwd_send),
        (coefs.at[1:], coef_send),
        (xn.at[0 : 3 * ff], core_send),
        (xn.at[0 : 3 * ff], cross_send),
        (xn.at[0 : 3 * ff], relay_send),
        (y.at[:, 0:ring_rows], sum_r_send),
        (y.at[:, 0:ring_rows], sum_l_send),
    ):
        remote(ref, ref, sem, sem, nxt).wait_send()
    for copy in [kvr["x"], *q_copies, *mixes]:
        copy.wait_send()
    with jax.named_scope("outs"):
        for copy in outs:
            copy.wait()


def on_device_fused(
    q_latent,
    kv_latent,
    rope_key,
    q_gain,
    kv_gain,
    w_query,
    w_query_rot,
    w_key,
    w_value,
    w_mix_out,
    expert_input,
    ffn_gain,
    expert_ids,
    route_weights,
    w_gate_exp,
    w_up_exp,
    w_down_exp,
):
    count = lax.axis_size("ep")
    chunks = 8
    rows, depth = expert_input.shape
    ff = w_gate_exp.shape[2]
    heads = w_key.shape[1] // NOPE
    rank = kv_latent.shape[1]
    q_rank = q_latent.shape[1]
    group_rows = 4 * rows
    half = count // 2
    width = depth // chunks
    pieces = 4 + chunks
    head_lanes = heads * LANES
    kv_width = rank + LANES
    half_width = ROPE // 2
    frequency = np.float32(rope_base) ** (-np.arange(half_width, dtype=np.float32) / half_width)
    frequency = jnp.asarray(np.tile(frequency, LANES // half_width)[None, :], jnp.float32)
    bf16, f32 = jnp.bfloat16, jnp.float32
    dma = pltpu.SemaphoreType.DMA
    vmem = pl.BlockSpec(memory_space=pltpu.VMEM)
    hbm = pl.BlockSpec(memory_space=pl.ANY)
    both = pl.pallas_call(
        functools.partial(layer_kernel, count, chunks),
        out_shape=jax.ShapeDtypeStruct((2, rows, depth), bf16),
        in_specs=[vmem] * 5 + [hbm] * 5 + [vmem, hbm, vmem, vmem, vmem] + [hbm] * 3,
        out_specs=hbm,
        scratch_shapes=[
            pltpu.VMEM((rows, depth), bf16),
            pltpu.VMEM(w_query.shape, bf16),
            pltpu.VMEM(w_query_rot.shape, bf16),
            pltpu.VMEM(w_key.shape, bf16),
            pltpu.VMEM(w_value.shape, bf16),
            pltpu.VMEM(w_mix_out.shape, bf16),
            pltpu.VMEM((rows, depth), bf16),
            pltpu.VMEM((rows, depth), bf16),
            pltpu.VMEM((group_rows, LANES), f32),
            pltpu.VMEM((group_rows, LANES), f32),
            pltpu.VMEM((count, rows), f32),
            pltpu.VMEM((group_rows, q_rank), bf16),
            pltpu.VMEM((q_rank, 2 * head_lanes), bf16),
            pltpu.VMEM((group_rows, head_lanes), bf16),
            pltpu.VMEM((count, group_rows, kv_width), bf16),
            pltpu.VMEM((kv_width, head_lanes), bf16),
            pltpu.VMEM((heads * VR, kv_width), bf16),
            pltpu.VMEM((group_rows, head_lanes), bf16),
            pltpu.VMEM((heads, VR, group_rows), bf16),
            pltpu.VMEM((heads, 1, group_rows), f32),
            pltpu.VMEM((heads, VR, group_rows), f32),
            pltpu.VMEM((heads * VD, group_rows), bf16),
            pltpu.VMEM((4, rows, depth), bf16),
            pltpu.VMEM((2, rows, depth), bf16),
            pltpu.VMEM((rows, depth), bf16),
            pltpu.VMEM((count, rows, depth), bf16),
            pltpu.VMEM((count * rows, depth), bf16),
            pltpu.VMEM((4, 2, 2, depth, ff // 2), bf16),
            pltpu.VMEM((chunks, 4 * ff, width), bf16),
            pltpu.VMEM((count * rows, 4 * ff), bf16),
            pltpu.VMEM((chunks, count * rows, width), bf16),
            pltpu.VMEM((chunks, half, rows, width), bf16),
            pltpu.VMEM((chunks, half, rows, width), bf16),
            pltpu.VMEM((count, count, rows), f32),
            pltpu.VMEM((count * rows, 1), f32),
            dma((3,)),
            dma((3,)),
            dma((2,)),
            dma,
            dma((half, 2)),
            dma,
            dma((half, 2)),
            dma,
            dma((count, 2)),
            dma((3,)),
            dma((3,)),
            dma((6,)),
            dma((chunks + 1,)),
            dma((pieces,)),
            dma,
            dma,
            dma,
            dma((half, 2)),
            dma,
            dma((half, 2)),
            dma,
            dma((pieces,)),
            dma,
            dma((pieces,)),
            dma,
            dma((pieces,)),
            dma,
            dma((chunks, half)),
            dma,
            dma((chunks, half)),
        ],
        compiler_params=pltpu.CompilerParams(
            collective_id=0, has_side_effects=True, vmem_limit_bytes=63 * 1024 * 1024
        ),
        cost_estimate=pl.CostEstimate(
            flops=6 * count * rows * depth * 4 * ff,
            bytes_accessed=12 * depth * ff * 2,
            transcendentals=count * rows * 4 * ff,
        ),
        name="layer",
    )(
        q_latent,
        kv_latent,
        rope_key.T,
        q_gain.reshape(1, -1),
        kv_gain.reshape(1, -1),
        w_query,
        w_query_rot,
        w_key,
        w_value,
        w_mix_out,
        frequency,
        expert_input,
        ffn_gain.reshape(1, -1),
        expert_ids.T,
        route_weights.T,
        w_gate_exp,
        w_up_exp,
        w_down_exp,
    )
    return both[0], both[1]


def fits(mesh):
    ep, tp = mesh.shape["ep"], mesh.shape["tp"]
    return tp == 4 and ep == 2 * tp


def solution(mesh):
    return jax.shard_map(
        on_device_fused if fits(mesh) else on_device_plain,
        mesh=mesh,
        in_specs=(
            P(("ep", "tp"), None),
            P(("ep", "tp"), None),
            P(("ep", "tp"), None),
            P(),
            P(),
            P(None, "tp"),
            P(None, "tp"),
            P(None, "tp"),
            P(None, "tp"),
            P("tp", None),
            P(("ep", "tp"), None),
            P(),
            P(("ep", "tp"), None),
            P(("ep", "tp"), None),
            P("ep", None, "tp"),
            P("ep", None, "tp"),
            P("ep", "tp", None),
        ),
        out_specs=(P(("ep", "tp"), None), P(("ep", "tp"), None)),
        check_vma=False,
    )
```
